32 devices in a mesh: sp: 8 (over z, x), tp: 4 (over y, core).
Axes of the slice: x: 2, y: 2, z: 4, core: 2. Of those that a mesh axis runs over, the one named last changes fastest.
Arguments:
- incoming_residual_stream: bfloat16 [4096, 2048], P(('sp', 'tp')), may hold values from -6 to 6
- result_valve: bfloat16 [4096, 2048], P('sp', 'tp'), may hold values from -6 to 6
- channel_feed_matrix: bfloat16 [4096, 2048], P('sp', 'tp'), may hold values from -6 to 6
- memory_feed_matrix: bfloat16 [4096, 512], P('sp', 'tp'), may hold values from -6 to 6
- memory_query_matrix: bfloat16 [4096, 512], P('sp', 'tp'), may hold values from -6 to 6
- unsoftened_deltas: float32 [4096, 32], P('sp', 'tp'), may hold values from -2.7 to 2.7
- delta_offset: float32 [32], P('tp'), may hold values from -4.5 to -3.5
- channel_fading_speed: float32 [32], P('tp'), as said below
- extra_log_fading: float32 [4096, 32], P('sp', 'tp'), may hold values from -0.7 to 0
- bypass_factor: float32 [32], P('tp'), may hold values from 0.1 to 1.9
- channel_feed_kernel: bfloat16 [4, 2048], P(None, 'tp'), may hold values from -3 to 3
- memory_feed_kernel: bfloat16 [4, 512], P(None, 'tp'), may hold values from -3 to 3
- memory_query_kernel: bfloat16 [4, 512], P(None, 'tp'), may hold values from -3 to 3
- cluster_scaling_vector: float32 [2048], P('tp'), may hold values from 0.1 to 1.9
- mixer_result_matrix: bfloat16 [2048, 2048], P('tp'), may hold values from -0.125 to 0.125
- initial_scaling_vector: float32 [2048], replicated, may hold values from 0.1 to 1.9
- valve_matrix: bfloat16 [2048, 5632], P('sp', 'tp'), may hold values from -0.125 to 0.125
- widen_matrix: bfloat16 [2048, 5632], P('sp', 'tp'), may hold values from -0.125 to 0.125
- shrink_matrix: bfloat16 [5632, 2048], P('tp', 'sp'), may hold values from -0.078125 to 0.078125
- valve_filter_kernel: bfloat16 [3, 5632], P(None, 'tp'), may hold values from -3.5 to 3.5
- widen_filter_kernel: bfloat16 [3, 5632], P(None, 'tp'), may hold values from -3.5 to 3.5
- latter_scaling_vector: float32 [2048], replicated, may hold values from 0.1 to 1.9
Outputs:
- layer_out: bfloat16 [4096, 2048], P(('sp', 'tp'))
The draws below stay inside these ranges and needn't reach their ends.
Inputs may be any that keep to these rules, and one draw needn't show every extreme that they name: `channel_fading_speed`: positive.
All inputs are finite; a program needn't handle non-finite values.
Results may differ from the reference program's by a relative error of at most 0.02.
Values may be sent and summed in bfloat16 or wider, within the bound.
A program may use at most 128 MiB of HBM per device.

```python
import math
import jax
import jax.numpy as jnp
from jax import lax

D = 2048
HEADS = 32
HEAD_DIM = 64
GROUPS = 4
STATE = 128
FF = 5632
CONV = 4
FCONV = 3
BLOCK = 128
TOK_DEV = 512
INNER = 2048
TOKENS = 4096
N_TP = 4


def draw_unsoftened_deltas(key, part):
    noise_key = jax.random.fold_in(key, 11)
    block_key = jax.random.fold_in(key, 12)
    centred_part = jnp.clip(0.5 * jax.random.normal(noise_key, (TOKENS, HEADS), jnp.float32), -2.0, 2.0)
    shifts = jax.random.uniform(block_key, (TOKENS // TOK_DEV, 1), jnp.float32, -0.7, 0.7)
    return centred_part + jnp.repeat(shifts, TOK_DEV, axis=0)


def draw_channel_fading_speed(key, part):
    slow_share = 0.5
    slow_mask = jax.random.uniform(jax.random.fold_in(key, 21), (HEADS,), jnp.float32) < slow_share
    fast_rate = jnp.exp(jax.random.uniform(jax.random.fold_in(key, 22), (HEADS,), jnp.float32, 0.0, math.log(4.0)))
    slow_rate = jax.random.uniform(jax.random.fold_in(key, 23), (HEADS,), jnp.float32, 10.0, 30.0) / TOKENS
    return jnp.where(slow_mask, slow_rate, fast_rate)


def draw_extra_log_fading(key, part):
    hits = jax.random.uniform(jax.random.fold_in(key, 31), (TOKENS, HEADS), jnp.float32) < 4.0 / TOKENS
    drops = jnp.log(jax.random.uniform(jax.random.fold_in(key, 32), (TOKENS, HEADS), jnp.float32, 0.5, 0.8))
    return jnp.where(hits, drops, 0.0)


def block_levels(key, dims, cuts, least, largest):
    level = 1.0
    for axis_at, shards_of in cuts:
        heights = jax.random.uniform(jax.random.fold_in(jax.random.fold_in(key, 6), axis_at), (shards_of,), jnp.float32, least / len(cuts), largest / len(cuts))
        level = level * jnp.repeat(jnp.exp(heights), dims[axis_at] // shards_of).reshape((-1,) + (1,) * (len(dims) - 1 - axis_at))
    return level


def noise(rng, dims, scale, limit, cuts=(), held_as=jnp.bfloat16):
    result = jax.random.normal(rng, dims, jnp.float32) * scale
    if len(cuts) > 0:
        result = block_levels(rng, dims, cuts, -0.22, 0.18) * result
    return jnp.clip(result, min=-limit, max=limit).astype(held_as)


def setup_inputs(seed: int = 0) -> dict:
    keys = jax.random.split(jax.random.key(seed), 23)
    incoming_residual_stream = noise(keys[0], (TOKENS, D), 1.0, 6.0, ((0, 32),))
    result_valve = noise(keys[1], (TOKENS, INNER), 1.0, 6.0, ((0, 8), (1, 4)))
    channel_feed_matrix = noise(keys[2], (TOKENS, INNER), 1.0, 6.0, ((0, 8), (1, 4)))
    memory_feed_matrix = noise(keys[3], (TOKENS, GROUPS * STATE), 1.0, 6.0, ((0, 8), (1, 4)))
    memory_query_matrix = noise(keys[4], (TOKENS, GROUPS * STATE), 1.0, 6.0, ((0, 8), (1, 4)))
    unsoftened_deltas = draw_unsoftened_deltas(jax.random.fold_in(keys[22], 71), 0)
    delta_offset = jnp.clip(-4.5 + 1.0 * jax.random.uniform(keys[6], (HEADS,), jnp.float32) ** block_levels(keys[6], (HEADS,), ((0, 4),), -0.2, 0.2), -4.5, -3.5)
    channel_fading_speed = draw_channel_fading_speed(jax.random.fold_in(keys[22], 71), 0)
    extra_log_fading = draw_extra_log_fading(jax.random.fold_in(keys[22], 71), 0)
    bypass_factor = jnp.clip(1.0 + 0.18 * jax.random.normal(keys[9], (HEADS,), jnp.float32), 0.1, 1.9)
    channel_feed_kernel = noise(keys[10], (CONV, INNER), CONV ** -0.5, 3.0, ((1, 4),))
    memory_feed_kernel = noise(keys[11], (CONV, GROUPS * STATE), CONV ** -0.5, 3.0, ((1, 4),))
    memory_query_kernel = noise(keys[12], (CONV, GROUPS * STATE), CONV ** -0.5, 3.0, ((1, 4),))
    cluster_scaling_vector = jnp.clip(1.0 + 0.18 * jax.random.normal(keys[13], (INNER,), jnp.float32), 0.1, 1.9)
    mixer_result_matrix = noise(keys[14], (INNER, D), INNER ** -0.5, 0.125, ((0, 4),))
    initial_scaling_vector = jnp.clip(1.0 + 0.18 * jax.random.normal(keys[15], (D,), jnp.float32), 0.1, 1.9)
    valve_matrix = noise(keys[16], (D, FF), D ** -0.5, 0.125, ((0, 8), (1, 4)))
    widen_matrix = noise(keys[17], (D, FF), D ** -0.5, 0.125, ((0, 8), (1, 4)))
    shrink_matrix = noise(keys[18], (FF, D), FF ** -0.5, 0.078125, ((0, 4), (1, 8)))
    valve_filter_kernel = noise(keys[19], (FCONV, FF), FCONV ** -0.5, 3.5, ((1, 4),))
    widen_filter_kernel = noise(keys[20], (FCONV, FF), FCONV ** -0.5, 3.5, ((1, 4),))
    latter_scaling_vector = jnp.clip(1.0 + 0.18 * jax.random.normal(keys[21], (D,), jnp.float32), 0.1, 1.9)
    return {"incoming_residual_stream": incoming_residual_stream, "result_valve": result_valve, "channel_feed_matrix": channel_feed_matrix, "memory_feed_matrix": memory_feed_matrix, "memory_query_matrix": memory_query_matrix, "unsoftened_deltas": unsoftened_deltas, "delta_offset": delta_offset, "channel_fading_speed": channel_fading_speed, "extra_log_fading": extra_log_fading, "bypass_factor": bypass_factor, "channel_feed_kernel": channel_feed_kernel, "memory_feed_kernel": memory_feed_kernel, "memory_query_kernel": memory_query_kernel, "cluster_scaling_vector": cluster_scaling_vector, "mixer_result_matrix": mixer_result_matrix, "initial_scaling_vector": initial_scaling_vector, "valve_matrix": valve_matrix, "widen_matrix": widen_matrix, "shrink_matrix": shrink_matrix, "valve_filter_kernel": valve_filter_kernel, "widen_filter_kernel": widen_filter_kernel, "latter_scaling_vector": latter_scaling_vector}


EPSILON = 1e-05
ALPHA = 2.0 ** 0.25
HIGHEST = lax.Precision.HIGHEST

def causal_conv(signal, before, tap_weights):
    tap_count = tap_weights.shape[0]
    row_count = signal.shape[0]
    padded = jnp.concatenate([before, signal], axis=0).astype(jnp.float32)
    running = jnp.zeros(signal.shape, jnp.float32)
    for tap_index in range(tap_count):
        running = running + tap_weights[tap_index].astype(jnp.float32) * padded[tap_index:tap_index + row_count]
    return running

def zero_rim(signal, tap_count):
    return jnp.zeros((tap_count - 1, signal.shape[1]), signal.dtype)

def layer_norm(values, scales):
    row_mean = lax.optimization_barrier(jnp.mean(values, axis=-1, keepdims=True))
    centred = values - row_mean
    spread = lax.optimization_barrier(jnp.mean(centred * centred, axis=-1, keepdims=True))
    return centred * lax.rsqrt(spread + EPSILON) * scales

def block_sum(activations, weights, pieces):
    slice_width = activations.shape[1] // pieces
    running = jnp.zeros((activations.shape[0], weights.shape[1]), jnp.float32)
    for piece_index in range(pieces):
        lower = piece_index * slice_width
        partial_value = jnp.dot(activations[:, lower:lower + slice_width], weights[lower:lower + slice_width], preferred_element_type=jnp.float32)
        rounded = lax.optimization_barrier(partial_value.astype(jnp.bfloat16))
        running = running + rounded.astype(jnp.float32)
    return running

def ssd_block(state_now, inputs):
    x_blk, b_blk, c_blk, decay_blk = inputs
    cum_decay = jnp.cumsum(decay_blk, axis=0)
    block_len = decay_blk.shape[0]
    causal = jnp.tril(jnp.ones((block_len, block_len), dtype=bool))
    between = cum_decay[:, None] - cum_decay[None, :]
    lag = jnp.exp(jnp.where(causal[:, :, None, None], between, -jnp.inf))
    affinity = jnp.einsum('lgn,sgn->lsg', c_blk, b_blk, precision=HIGHEST)
    mixing = affinity[..., None] * lag
    within = jnp.einsum('lsgh,sghp->lghp', mixing, x_blk, precision=HIGHEST)
    carried = jnp.einsum('lgn,ghpn->lghp', c_blk, state_now, precision=HIGHEST) * jnp.exp(cum_decay)[..., None]
    to_end = jnp.exp(cum_decay[-1] - cum_decay)
    fresh = jnp.einsum('lgn,lghp->ghpn', b_blk, x_blk * to_end[..., None], precision=HIGHEST)
    state_next = state_now * jnp.exp(cum_decay[-1])[..., None, None] + fresh
    return (state_next, within + carried)

def reference(incoming_residual_stream, result_valve, channel_feed_matrix, memory_feed_matrix, memory_query_matrix, unsoftened_deltas, delta_offset, channel_fading_speed, extra_log_fading, bypass_factor, channel_feed_kernel, memory_feed_kernel, memory_query_kernel, cluster_scaling_vector, mixer_result_matrix, initial_scaling_vector, valve_matrix, widen_matrix, shrink_matrix, valve_filter_kernel, widen_filter_kernel, latter_scaling_vector):
    group_heads = HEADS // GROUPS
    x_act = jax.nn.silu(causal_conv(channel_feed_matrix, zero_rim(channel_feed_matrix, CONV), channel_feed_kernel)).astype(jnp.bfloat16)
    b_act = jax.nn.silu(causal_conv(memory_feed_matrix, zero_rim(memory_feed_matrix, CONV), memory_feed_kernel)).astype(jnp.bfloat16)
    c_act = jax.nn.silu(causal_conv(memory_query_matrix, zero_rim(memory_query_matrix, CONV), memory_query_kernel)).astype(jnp.bfloat16)
    channel_delta_amount = jax.nn.softplus(unsoftened_deltas + delta_offset[None, :])
    log_fading_amount = extra_log_fading - channel_fading_speed[None, :] * channel_delta_amount
    block_count = TOKENS // BLOCK
    x_heads = x_act.astype(jnp.float32).reshape(TOKENS, GROUPS, group_heads, HEAD_DIM)
    x_scaled = x_heads * channel_delta_amount.reshape(TOKENS, GROUPS, group_heads)[..., None]
    x_blocks = x_scaled.reshape(block_count, BLOCK, GROUPS, group_heads, HEAD_DIM)
    b_blocks = b_act.astype(jnp.float32).reshape(block_count, BLOCK, GROUPS, STATE)
    c_blocks = c_act.astype(jnp.float32).reshape(block_count, BLOCK, GROUPS, STATE)
    decay_blocks = log_fading_amount.reshape(block_count, BLOCK, GROUPS, group_heads)
    initial = jnp.zeros((GROUPS, group_heads, HEAD_DIM, STATE), jnp.float32)
    _, mixed = lax.scan(ssd_block, initial, (x_blocks, b_blocks, c_blocks, decay_blocks))
    y_heads = mixed.reshape(TOKENS, GROUPS, group_heads, HEAD_DIM)
    y_heads = y_heads + bypass_factor.reshape(GROUPS, group_heads)[None, :, :, None] * x_heads
    gated = y_heads.reshape(TOKENS, GROUPS, INNER // GROUPS)
    gated = gated * jax.nn.silu(result_valve.astype(jnp.float32)).reshape(TOKENS, GROUPS, INNER // GROUPS)
    gated = gated * lax.rsqrt(lax.optimization_barrier(jnp.mean(gated * gated, axis=-1, keepdims=True)) + EPSILON)
    y_norm = (gated.reshape(TOKENS, INNER) * cluster_scaling_vector[None, :]).astype(jnp.bfloat16)
    mixer = block_sum(y_norm, mixer_result_matrix, N_TP)
    normed = layer_norm(ALPHA * incoming_residual_stream.astype(jnp.float32) + mixer, initial_scaling_vector).astype(jnp.bfloat16)
    gate_proj = jnp.dot(normed, valve_matrix, preferred_element_type=jnp.float32).astype(jnp.bfloat16)
    up_proj = jnp.dot(normed, widen_matrix, preferred_element_type=jnp.float32).astype(jnp.bfloat16)
    gate_conv = causal_conv(gate_proj, zero_rim(gate_proj, FCONV), valve_filter_kernel)
    up_conv = causal_conv(up_proj, zero_rim(up_proj, FCONV), widen_filter_kernel)
    hidden = (jax.nn.silu(gate_conv) * up_conv).astype(jnp.bfloat16)
    channel = block_sum(hidden, shrink_matrix, N_TP)
    return layer_norm(ALPHA * normed.astype(jnp.float32) + channel, latter_scaling_vector).astype(jnp.bfloat16)
```

```python
import functools
import jax
import jax.numpy as jnp
from jax import lax
from jax.experimental import pallas as pl
from jax.experimental.pallas import tpu as pltpu
from jax.sharding import PartitionSpec as P

HEADS = 32
HEAD_DIM = 64
GROUPS = 4
STATE = 128
CONV = 4
FCONV = 3
BLOCK = 128


EPSILON = 1e-05
ALPHA = 2.0**0.25
HIGHEST = lax.Precision.HIGHEST


def shifted(shard, axis, by):
    count = lax.axis_size(axis)
    pairs = [(i, i + by) for i in range(count) if 0 <= i + by < count]
    return lax.ppermute(shard, axis, pairs)


def entering(shard, axis, join, neutral):
    place = lax.axis_index(axis)
    gathered = jax.tree.map(
        lambda a, kind: lax.all_gather(a.astype(kind), axis), shard, (jnp.bfloat16, jnp.bfloat16)
    )
    state = jax.tree.map(lambda a, e: jnp.zeros_like(a) + jnp.asarray(e, a.dtype), shard, neutral)

    def one(lap, state):
        return join(
            state,
            jax.tree.map(
                lambda a, own: lax.dynamic_index_in_dim(a, lap, 0, False).astype(own.dtype),
                gathered,
                shard,
            ),
        )

    return lax.fori_loop(0, place, one, state)


def causal_conv(signal, before, tap_weights):
    tap_count = tap_weights.shape[0]
    row_count = signal.shape[0]
    padded = jnp.concatenate([before, signal], axis=0).astype(jnp.float32)
    running = jnp.zeros(signal.shape, jnp.float32)
    for tap_index in range(tap_count):
        running = (
            running
            + tap_weights[tap_index].astype(jnp.float32) * padded[tap_index : tap_index + row_count]
        )
    return running


def layer_norm(values, scales):
    row_mean = jnp.mean(values, axis=-1, keepdims=True)
    centred = values - row_mean
    spread = jnp.mean(centred * centred, axis=-1, keepdims=True)
    return centred * lax.rsqrt(spread + EPSILON) * scales


def combine_states(earlier_pair, later_pair):
    return (
        earlier_pair[0] * later_pair[1][..., None, None] + later_pair[0],
        earlier_pair[1] * later_pair[1],
    )


def chain_step(state_now, inputs):
    fresh_one, decay_one = inputs
    return (state_now * decay_one[..., None, None] + fresh_one, state_now)


def plain_shards(
    incoming_residual_stream,
    result_valve,
    channel_feed_matrix,
    memory_feed_matrix,
    memory_query_matrix,
    unsoftened_deltas,
    delta_offset,
    channel_fading_speed,
    extra_log_fading,
    bypass_factor,
    channel_feed_kernel,
    memory_feed_kernel,
    memory_query_kernel,
    cluster_scaling_vector,
    mixer_result_matrix,
    initial_scaling_vector,
    valve_matrix,
    widen_matrix,
    shrink_matrix,
    valve_filter_kernel,
    widen_filter_kernel,
    latter_scaling_vector,
):
    row_count = channel_feed_matrix.shape[0]
    inner_here = channel_feed_matrix.shape[1]
    group_count = memory_feed_matrix.shape[1] // STATE
    group_heads = HEADS // GROUPS
    block_count = row_count // BLOCK
    rim_rows = CONV - 1
    rim_x, rim_b, rim_c = shifted(
        (
            channel_feed_matrix[row_count - rim_rows :],
            memory_feed_matrix[row_count - rim_rows :],
            memory_query_matrix[row_count - rim_rows :],
        ),
        "sp",
        1,
    )
    x_act = jax.nn.silu(causal_conv(channel_feed_matrix, rim_x, channel_feed_kernel)).astype(
        jnp.bfloat16
    )
    b_act = jax.nn.silu(causal_conv(memory_feed_matrix, rim_b, memory_feed_kernel)).astype(
        jnp.bfloat16
    )
    c_act = jax.nn.silu(causal_conv(memory_query_matrix, rim_c, memory_query_kernel)).astype(
        jnp.bfloat16
    )
    channel_delta_amount = jax.nn.softplus(unsoftened_deltas + delta_offset[None, :])
    log_fading_amount = extra_log_fading - channel_fading_speed[None, :] * channel_delta_amount
    x_heads = x_act.astype(jnp.float32).reshape(row_count, group_count, group_heads, HEAD_DIM)
    x_scaled = (
        x_heads * channel_delta_amount.reshape(row_count, group_count, group_heads)[..., None]
    )
    b_full = b_act.astype(jnp.float32).reshape(row_count, group_count, STATE)
    c_full = c_act.astype(jnp.float32).reshape(row_count, group_count, STATE)
    decay_full = log_fading_amount.reshape(row_count, group_count, group_heads)
    x_blk = x_scaled.reshape(block_count, BLOCK, group_count, group_heads, HEAD_DIM)
    b_blk = b_full.reshape(block_count, BLOCK, group_count, STATE)
    c_blk = c_full.reshape(block_count, BLOCK, group_count, STATE)
    b_narrow = b_act.reshape(block_count, BLOCK, group_count, STATE)
    c_narrow = c_act.reshape(block_count, BLOCK, group_count, STATE)
    decay_blk = decay_full.reshape(block_count, BLOCK, group_count, group_heads)
    cum_decay = jnp.cumsum(decay_blk, axis=1)
    causal = jnp.tril(jnp.ones((BLOCK, BLOCK), dtype=bool))
    between = cum_decay[:, :, None] - cum_decay[:, None, :]
    lag = jnp.exp(jnp.where(causal[None, :, :, None, None], between, -jnp.inf))
    affinity = jnp.einsum("blgn,bsgn->blsg", c_narrow, b_narrow, preferred_element_type=jnp.float32)
    mixing = affinity[..., None] * lag
    within = jnp.einsum("blsgh,bsghp->blghp", mixing, x_blk, precision=HIGHEST)
    to_end = jnp.exp(cum_decay[:, -1:] - cum_decay)
    fresh = jnp.einsum("blgn,blghp->bghpn", b_blk, x_blk * to_end[..., None], precision=HIGHEST)
    block_decay = jnp.exp(cum_decay[:, -1])
    initial = jnp.zeros((group_count, group_heads, HEAD_DIM, STATE), jnp.float32)
    local_end, earlier = lax.scan(chain_step, initial, (fresh, block_decay))
    carried = (
        jnp.einsum("blgn,bghpn->blghp", c_blk, earlier, precision=HIGHEST)
        * jnp.exp(cum_decay)[..., None]
    )
    from_start = jnp.cumsum(decay_full, axis=0)
    incoming, _ = entering(
        (local_end, jnp.exp(from_start[-1])),
        "sp",
        combine_states,
        (jnp.zeros_like(local_end), jnp.ones_like(from_start[-1])),
    )
    arriving = (
        jnp.einsum("tgn,ghpn->tghp", c_full, incoming, precision=HIGHEST)
        * jnp.exp(from_start)[..., None]
    )
    y_heads = (within + carried).reshape(row_count, group_count, group_heads, HEAD_DIM) + arriving
    y_heads = y_heads + bypass_factor.reshape(group_count, group_heads)[None, :, :, None] * x_heads
    gated = y_heads.reshape(row_count, group_count, group_heads * HEAD_DIM)
    gated = gated * jax.nn.silu(result_valve.astype(jnp.float32)).reshape(
        row_count, group_count, group_heads * HEAD_DIM
    )
    gated = gated * lax.rsqrt(jnp.mean(gated * gated, axis=-1, keepdims=True) + EPSILON)
    y_norm = (gated.reshape(row_count, inner_here) * cluster_scaling_vector[None, :]).astype(
        jnp.bfloat16
    )
    mixer = lax.psum_scatter(
        jnp.dot(y_norm, mixer_result_matrix, preferred_element_type=jnp.float32).astype(
            jnp.bfloat16
        ),
        "tp",
        scatter_dimension=0,
        tiled=True,
    ).astype(jnp.float32)
    normed_own = layer_norm(
        ALPHA * incoming_residual_stream.astype(jnp.float32) + mixer, initial_scaling_vector
    ).astype(jnp.bfloat16)
    normed_all = lax.all_gather(normed_own, "tp", axis=0, tiled=True)
    gate_sum = jnp.dot(
        normed_all,
        lax.all_gather(valve_matrix, "sp", axis=0, tiled=True),
        preferred_element_type=jnp.float32,
    )
    up_sum = jnp.dot(
        normed_all,
        lax.all_gather(widen_matrix, "sp", axis=0, tiled=True),
        preferred_element_type=jnp.float32,
    )
    gate_proj = gate_sum.astype(jnp.bfloat16)
    up_proj = up_sum.astype(jnp.bfloat16)
    ffn_rows = FCONV - 1
    rim_gate, rim_up = shifted(
        (gate_proj[row_count - ffn_rows :], up_proj[row_count - ffn_rows :]), "sp", 1
    )
    gate_conv = causal_conv(gate_proj, rim_gate, valve_filter_kernel)
    up_conv = causal_conv(up_proj, rim_up, widen_filter_kernel)
    hidden = (jax.nn.silu(gate_conv) * up_conv).astype(jnp.bfloat16)
    channel_part = jnp.dot(
        hidden,
        lax.all_gather(shrink_matrix, "sp", axis=1, tiled=True),
        preferred_element_type=jnp.float32,
    )
    channel = lax.psum_scatter(
        channel_part.astype(jnp.bfloat16), "tp", scatter_dimension=0, tiled=True
    ).astype(jnp.float32)
    return layer_norm(
        ALPHA * normed_own.astype(jnp.float32) + channel, latter_scaling_vector
    ).astype(jnp.bfloat16)


MESH = pl.DeviceIdType.MESH
RIM = 16
FAN = 2
HALVES = 2


def silu(v):
    return v / (1.0 + jnp.exp(-v))


def layer_kernel(
    n_sp,
    n_tp,
    res_hbm,
    rv_hbm,
    xf_ref,
    bf_ref,
    cf_ref,
    dt_ref,
    doff_ref,
    fade_ref,
    elf_ref,
    byp_ref,
    xk_ref,
    bk_ref,
    ck_ref,
    csv_ref,
    mm_hbm,
    g1_ref,
    v_hbm,
    w_hbm,
    s_hbm,
    vk_ref,
    wk_ref,
    g2_ref,
    out_ref,
    v_all,
    w_all,
    s_all,
    rim_x,
    rim_b,
    rim_c,
    vk_other,
    wk_other,
    ext,
    x_act,
    b_act,
    c_act,
    step_ref,
    ld_ref,
    y_ref,
    efs_ref,
    base_ref,
    state_ref,
    st_send,
    dec_send,
    pair_send,
    pair_dec,
    st_recv,
    dec_recv,
    part,
    near_recv,
    side_send,
    side_recv,
    own_norm,
    recv2,
    normed,
    hidden,
    res_ref,
    rv_ref,
    mm_ref,
    late_sem,
    own_sem,
    w_recv,
    z_send,
    xo_send,
    do_send,
    xr_send,
    dr_send,
    rim_send,
    rim_recv,
    tap_send,
    tap_recv,
    st_ssem,
    st_rsem,
    a_send,
    a_recv,
    b_send,
    b_recv,
    ag_send,
    ag_recv,
    agr_send,
    halo_send,
    halo_recv,
    t3_send,
    t3_recv,
):
    f32, bf16 = jnp.float32, jnp.bfloat16
    rows, inner = xf_ref.shape
    heads = dt_ref.shape[0]
    own_rows = rows // n_tp
    width = mm_hbm.shape[1]
    ff = v_hbm.shape[1]
    depth = v_hbm.shape[0]
    cols = s_hbm.shape[1]
    blocks = rows // BLOCK
    planes = n_sp // FAN
    dests = planes // 2
    half = n_sp // 2
    me = lax.axis_index("sp")
    mt = lax.axis_index("tp")
    z, x = me // FAN, me % FAN
    y, c = mt // 2, mt % 2
    b = z % 2
    mate = z + 1 - 2 * b
    pair0 = z - b

    def dev(pz, px, py, pc):
        return (pz * FAN + px, py * 2 + pc)

    def remote(src, dst, send, recv, device):
        return pltpu.make_async_remote_copy(
            src_ref=src, dst_ref=dst, send_sem=send, recv_sem=recv, device_id=device, device_id_type=MESH
        )

    barrier = pltpu.get_barrier_semaphore()
    total_devices = n_sp * n_tp
    line = me * n_tp + mt
    for d in range(1, total_devices):
        who = (line + d) % total_devices
        pl.semaphore_signal(barrier, inc=1, device_id=(who // n_tp, who % n_tp), device_id_type=MESH)
    pl.semaphore_wait(barrier, total_devices - 1)

    units = [(kind, g) for kind in range(3) for g in range(HALVES)]
    sources = (v_hbm, w_hbm, s_hbm)

    def place(u, q):
        kind, g = units[u]
        size = (ff if kind == 2 else depth) // (2 * HALVES)
        return size, (q * HALVES + g) * size

    def own_piece(u, q):
        size, at = place(u, q)
        return sources[units[u][0]].at[pl.ds(pl.multiple_of(at, 16), size)]

    def slot(u, q, who):
        size, at = place(u, q)
        kind = units[u][0]
        if kind == 2:
            return s_all.at[who, pl.ds(pl.multiple_of(at, 16), size)]
        whole = v_all if kind == 0 else w_all
        return whole.at[pl.ds(pl.multiple_of(who * depth + at, 16), size)]

    def landed(u, q, who):
        here = slot(u, q, who)
        return remote(here, here, do_send.at[0, 0], w_recv.at[u, q, who], dev(z, x, y, 1 - c))

    def z_copy(u, q, j):
        return remote(
            own_piece(u, q),
            slot(u, q, me),
            z_send.at[u, q, j],
            w_recv.at[u, q, me],
            dev(2 * j + c, x, y, q),
        )

    def xo_copy(u, q):
        return remote(
            own_piece(u, q), slot(u, q, me), xo_send.at[u, q], w_recv.at[u, q, me], dev(z, 1 - x, y, q)
        )

    def do_copy(u, q):
        return remote(
            own_piece(u, q), slot(u, q, me), do_send.at[u, q], w_recv.at[u, q, me], dev(z, x, y, 1 - c)
        )

    def xr_copy(u, i):
        here = slot(u, c, plane_at(i) * FAN + x)
        return remote(
            here,
            here,
            xr_send.at[u, i],
            w_recv.at[u, c, plane_at(i) * FAN + x],
            dev(z, 1 - x, y, c),
        )

    def dr_copy(u, who):
        here = slot(u, c, who)
        return remote(here, here, dr_send.at[u, who], w_recv.at[u, c, who], dev(z, x, y, 1 - c))

    def plane_at(i):
        if i == 0:
            return z
        low = jnp.where(z < planes // 2, z, planes - 1 - z)
        got = jnp.where(i - 1 < low, i - 1, i)
        return jnp.where(z < planes // 2, got, planes - 1 - got)

    def send_z(which):
        for u in which:
            for q in range(2):
                for j in range(dests):

                    @pl.when(2 * j + c != z)
                    def _(u=u, q=q, j=j):
                        z_copy(u, q, j).start()

    def send_xo(which):
        @pl.when(c == b)
        def _():
            for u in which:
                for q in range(2):
                    xo_copy(u, q).start()

    def relay_col(u, picks=None):
        for i in picks or range(1, planes):
            who = plane_at(i) * FAN + x
            landed(u, c, who).wait_recv()
            xr_copy(u, i).start()
            dr_copy(u, who).start()

    def relay_x(u, picks=None):
        for i in picks or range(planes):
            who = plane_at(i) * FAN + 1 - x
            landed(u, c, who).wait_recv()
            dr_copy(u, who).start()

    def other_half(us, who):
        for u in us:
            landed(u, 1 - c, who).wait_recv()

    def own_block(us):
        @pl.when(c != b)
        def _():
            for u in us:
                for q in range(2):
                    landed(u, q, me).wait_recv()

    rim_copies = []
    for i, (src, dst) in enumerate(((xf_ref, rim_x), (bf_ref, rim_b), (cf_ref, rim_c))):
        rim_copies.append(
            remote(
                src.at[pl.ds(rows - RIM, RIM)],
                dst,
                rim_send.at[i],
                rim_recv.at[i],
                ((me + 1) % n_sp, mt),
            )
        )
        rim_copies[-1].start()
    tap_copies = [
        remote(src, dst, tap_send.at[i], tap_recv.at[i], dev(z, x, y, 1 - c))
        for i, (src, dst) in enumerate(((vk_ref, vk_other), (wk_ref, wk_other)))
    ]
    for copy in tap_copies:
        copy.start()
    send_z([0])
    send_xo([0, 1, 2, 3])

    own_copies = []
    for kind in range(3):
        dst = s_all.at[me] if kind == 2 else (v_all, w_all)[kind].at[
            pl.ds(pl.multiple_of(me * depth, 16), depth)
        ]
        own_copies.append(pltpu.make_async_copy(sources[kind], dst, own_sem.at[kind]))

    @pl.when(c == b)
    def _():
        for u in range(len(units)):
            for q in range(2):
                do_copy(u, q).start()
        for copy in own_copies:
            copy.start()

    late = [
        pltpu.make_async_copy(src, dst, late_sem.at[i])
        for i, (src, dst) in enumerate(((rv_hbm, rv_ref), (mm_hbm, mm_ref), (res_hbm, res_ref)))
    ]
    for copy in late:
        copy.start()

    eye = lax.broadcasted_iota(jnp.int32, (heads, heads), 0) == lax.broadcasted_iota(
        jnp.int32, (heads, heads), 1
    )

    def column(a):
        return jnp.sum(jnp.where(eye, a[...], 0.0), axis=1, keepdims=True)

    raw = dt_ref[...] + column(doff_ref)
    step_ref[...] = jnp.maximum(raw, 0.0) + jnp.log1p(jnp.exp(-jnp.abs(raw)))
    ld_ref[...] = elf_ref[...] - column(fade_ref) * step_ref[...]

    for copy in rim_copies:
        copy.wait_recv()
    first = me == 0
    for rim, feed, taps, act in (
        (rim_x, xf_ref, xk_ref, x_act),
        (rim_b, bf_ref, bk_ref, b_act),
        (rim_c, cf_ref, ck_ref, c_act),
    ):
        for lo in range(0, feed.shape[1], 128):
            here = slice(lo, lo + 128)
            edge = rim[:, here].astype(f32)
            ext[0:RIM, :] = jnp.where(first, jnp.zeros_like(edge), edge)
            ext[RIM:, :] = feed[:, here].astype(f32)
            tap = taps[:, here].astype(f32)
            total = jnp.zeros((rows, 128), f32)
            for k in range(CONV):
                start = RIM - (CONV - 1) + k
                total = total + tap[k : k + 1] * ext[start : start + rows, :]
            act[:, here] = silu(total).astype(bf16)

    li = lax.broadcasted_iota(jnp.int32, (BLOCK, BLOCK), 0)
    si = lax.broadcasted_iota(jnp.int32, (BLOCK, BLOCK), 1)
    causal = li >= si
    lower = jnp.where(causal, 1.0, 0.0).astype(f32)
    upper = jnp.where(li <= si, 1.0, 0.0).astype(f32)
    spread = jnp.where(
        lax.broadcasted_iota(jnp.int32, (heads, inner), 1) // HEAD_DIM
        == lax.broadcasted_iota(jnp.int32, (heads, inner), 0),
        1.0,
        0.0,
    ).astype(f32)
    near = lax.broadcasted_iota(jnp.int32, (BLOCK, 2 * HEAD_DIM), 1) < HEAD_DIM

    def widen(a):
        return jnp.dot(a, spread, precision=HIGHEST, preferred_element_type=f32)

    state_ref[...] = jnp.zeros_like(state_ref)
    base_ref[...] = jnp.zeros_like(base_ref)
    skip = widen(byp_ref[...])

    def scan_block(i, carry):
        at = pl.ds(pl.multiple_of(i * BLOCK, BLOCK), BLOCK)
        ld = ld_ref[:, at]
        cum = lax.dot_general(
            lower, ld, (((1,), (1,)), ((), ())), precision=HIGHEST, preferred_element_type=f32
        )
        cum_t = jnp.dot(ld, upper, precision=HIGHEST, preferred_element_type=f32)
        last = cum[BLOCK - 1 : BLOCK, :]
        xx = x_act[at, :].astype(f32)
        bb = b_act[at, :]
        cc = c_act[at, :]
        xs = xx * lax.dot_general(
            step_ref[:, at],
            spread,
            (((0,), (0,)), ((), ())),
            precision=HIGHEST,
            preferred_element_type=f32,
        )
        xs16 = xs.astype(bf16)
        aff = lax.dot_general(
            cc, bb, (((1,), (1,)), ((), ())), preferred_element_type=f32
        )
        yy = (
            jnp.dot(cc, state_ref[...].astype(bf16), preferred_element_type=f32)
            * widen(jnp.exp(cum))
            + skip * xx
        )
        for pair in range(heads // 2):
            at_pair = slice(pair * 2 * HEAD_DIM, (pair + 1) * 2 * HEAD_DIM)
            both = []
            for h in (2 * pair, 2 * pair + 1):
                gap = cum[:, h : h + 1] - cum_t[h : h + 1, :]
                lag = jnp.exp(jnp.where(causal, gap, -1e30))
                both.append(
                    jnp.dot(
                        (aff * lag).astype(bf16), xs16[:, at_pair], preferred_element_type=f32
                    )
                )
            y_ref[at, at_pair] = yy[:, at_pair] + jnp.where(near, both[0], both[1])
        fresh = lax.dot_general(
            bb,
            (xs * widen(jnp.exp(last - cum))).astype(bf16),
            (((0,), (0,)), ((), ())),
            preferred_element_type=f32,
        )
        state_ref[...] = state_ref[...] * widen(jnp.exp(last)) + fresh
        base = base_ref[0:1, :]
        efs_ref[at, :] = jnp.exp(base + cum)
        base_ref[0:1, :] = base + last
        return carry

    lax.fori_loop(0, blocks, scan_block, 0)
    st_send[...] = state_ref[...].astype(bf16)
    dec_send[...] = jnp.broadcast_to(base_ref[0:1, :], dec_send.shape)
    odd = me % 2
    partner = me + 1 - 2 * odd

    def state_copies(d):
        pair = d > 0
        return [
            remote(
                src,
                dst.at[d],
                st_ssem.at[d, i],
                st_rsem.at[d, i],
                ((me + 2 * d) % n_sp if pair else partner, mt),
            )
            for i, (src, dst) in enumerate(
                ((pair_send if pair else st_send, st_recv), (pair_dec if pair else dec_send, dec_recv))
            )
        ]

    for copy in state_copies(0):
        copy.start()
    send_xo([4, 5])
    for copy in state_copies(0):
        copy.wait_recv()
    own_dec = widen(jnp.exp(dec_send[0:1, :]))
    beside_dec = widen(jnp.exp(dec_recv[0, 0:1, :]))
    beside = st_recv[0].astype(f32)
    later = odd == 1
    pair_send[...] = jnp.where(
        later, state_ref[...] + beside * own_dec, state_ref[...] * beside_dec + beside
    ).astype(bf16)
    pair_dec[...] = dec_send[...] + dec_recv[0]
    state_ref[...] = jnp.zeros_like(state_ref)
    for d in range(1, half):

        @pl.when(me + 2 * d < n_sp)
        def _(d=d):
            for copy in state_copies(d):
                copy.start()

    send_z([1, 2])
    relay_col(0)
    for d in range(half - 1, 0, -1):

        @pl.when(me >= 2 * d)
        def _(d=d):
            for copy in state_copies(d):
                copy.wait_recv()
            state_ref[...] = state_ref[...] * widen(
                jnp.exp(dec_recv[d, 0:1, :])
            ) + st_recv[d].astype(f32)

    @pl.when(odd == 1)
    def _():
        state_ref[...] = state_ref[...] * widen(jnp.exp(dec_recv[0, 0:1, :])) + st_recv[
            0
        ].astype(f32)

    for copy in late:
        copy.wait()

    def project_block(i, carry):
        at = pl.ds(pl.multiple_of(i * BLOCK, BLOCK), BLOCK)
        yy = y_ref[at, :] + jnp.dot(
            c_act[at, :], state_ref[...].astype(bf16), preferred_element_type=f32
        ) * widen(efs_ref[at, :])
        gated = yy * silu(rv_ref[at, :].astype(f32))
        gated = gated * lax.rsqrt(jnp.mean(gated * gated, axis=-1, keepdims=True) + EPSILON)
        y_norm = (gated * csv_ref[...]).astype(bf16)
        part[at, :] = jnp.dot(y_norm, mm_ref[...], preferred_element_type=f32).astype(bf16)
        return carry

    def rows_of(t):
        return pl.ds(pl.multiple_of(t * own_rows, own_rows), own_rows)

    def near_copy(py):
        return remote(
            part.at[rows_of(py * 2 + 1 - c)],
            near_recv.at[py],
            a_send.at[py],
            a_recv.at[py],
            dev(z, x, y, 1 - c),
        )

    halfway = blocks // 2
    lax.fori_loop((1 - y) * halfway, (2 - y) * halfway, project_block, 0)
    near_copy(1 - y).start()
    lax.fori_loop(y * halfway, (y + 1) * halfway, project_block, 0)
    near_copy(y).start()

    strips = 2
    strip = own_rows // strips

    def side_copy(k):
        at = pl.ds(k * strip, strip)
        return remote(
            side_send.at[at], side_recv.at[at], b_send.at[k], b_recv.at[k], dev(z, x, 1 - y, c)
        )

    near_copy(1 - y).wait_recv()
    for k in range(strips):
        away = pl.ds(pl.multiple_of(((1 - y) * 2 + c) * own_rows + k * strip, strip), strip)
        side_send[k * strip : (k + 1) * strip, :] = (
            part[away, :].astype(f32) + near_recv[1 - y, k * strip : (k + 1) * strip, :].astype(f32)
        ).astype(bf16)
        side_copy(k).start()
    near_copy(y).wait_recv()
    relay_col(1)

    def ag_copies(k):
        lo = pl.ds(k * strip, strip)
        to = normed.at[pl.ds(pl.multiple_of(RIM + mt * own_rows + k * strip, RIM), strip)]
        return [
            remote(own_norm.at[lo], to, ag_send.at[i, k], ag_recv.at[mt, k], device)
            for i, device in enumerate((dev(mate, x, y, b), dev(z, x, 1 - y, b), dev(z, x, y, b)))
        ]

    for k in range(strips):
        side_copy(k).wait_recv()
        lo = slice(k * strip, (k + 1) * strip)
        mine = pl.ds(pl.multiple_of(mt * own_rows + k * strip, strip), strip)
        mixer = (
            part[mine, :].astype(f32)
            + near_recv[y, lo, :].astype(f32)
            + side_recv[lo, :].astype(f32)
        )
        own_norm[lo, :] = layer_norm(
            ALPHA * res_ref[lo, :].astype(f32) + mixer, g1_ref[...]
        ).astype(bf16)
        copies = ag_copies(k)
        copies[0].start()
        copies[1].start()

        @pl.when(c != b)
        def _(copies=copies):
            copies[2].start()

        @pl.when(c == b)
        def _(k=k, lo=lo):
            normed[pl.ds(pl.multiple_of(RIM + mt * own_rows + k * strip, RIM), strip), :] = own_norm[
                lo, :
            ]

    nxt = me + 1
    nz, nx = nxt // FAN, nxt % FAN
    tail = jnp.logical_and(mt == n_tp - 1, nxt < n_sp)
    halo_copies = [
        remote(
            own_norm.at[pl.ds(own_rows - RIM, RIM)],
            normed.at[pl.ds(0, RIM)],
            halo_send.at[i],
            halo_recv,
            dev(jnp.minimum(nz, planes - 1) // 2 * 2 + i // 2, nx, i % 2, nz % 2),
        )
        for i in range(4)
    ]

    @pl.when(tail)
    def _():
        for copy in halo_copies:
            copy.start()

    send_z([3, 4, 5])

    def gathered(t, k):
        here = normed.at[pl.ds(pl.multiple_of(RIM + t * own_rows + k * strip, RIM), strip)]
        return remote(here, here, ag_send.at[0, 0], ag_recv.at[t, k], dev(z, x, y, 1 - c))

    def passed_on(pc, k):
        here = normed.at[pl.ds(pl.multiple_of(RIM + (y * 2 + pc) * own_rows + k * strip, RIM), strip)]
        return remote(here, here, agr_send.at[pc, k], ag_recv.at[y * 2 + pc, k], dev(z, x, 1 - y, c))

    seg = (pair0 + c) * FAN + x
    block_of = y * 2 + b

    relay_x(0)
    relay_x(1)
    relay_col(2)

    @pl.when(c != b)
    def _():
        for k in range(strips):
            for pc in range(2):
                gathered(y * 2 + pc, k).wait_recv()
                passed_on(pc, k).start()

    relay_x(2)
    relay_col(3)

    @pl.when(seg == 0)
    def _():
        normed[0:RIM, :] = jnp.zeros((RIM, width), bf16)

    @pl.when(seg > 0)
    def _():
        halo_copies[0].wait_recv()

    for k in range(strips):

        @pl.when(c == b)
        def _(k=k):
            gathered(y * 2 + 1 - c, k).wait_recv()

        for pc in range(2):
            gathered((1 - y) * 2 + pc, k).wait_recv()

    relay_x(3)

    @pl.when(c == b)
    def _():
        for copy in own_copies:
            copy.wait()

    own_block(range(4))

    def rest(who, carry):
        @pl.when(who != me)
        def _():
            other_half(range(4), who)

        return carry

    lax.fori_loop(0, n_sp, rest, 0)
    for copy in tap_copies:
        copy.wait()
    same = c == b

    def ffn_cols(at):
        feeds = normed[...]
        convs = []
        for weights, taps, others in ((v_all, vk_ref, vk_other), (w_all, wk_ref, wk_other)):
            proj = jnp.dot(feeds, weights[:, at], preferred_element_type=f32)
            proj = proj.astype(bf16).astype(f32)
            tap = jnp.where(same, taps[:, at].astype(f32), others[:, at].astype(f32))
            total = jnp.zeros((rows, proj.shape[1]), f32)
            for k in range(FCONV):
                start = RIM - (FCONV - 1) + k
                total = total + tap[k : k + 1] * proj[start : start + rows, :]
            convs.append(total)
        hidden[:, at] = (silu(convs[0]) * convs[1]).astype(bf16)

    chunk = 256
    full = ff // chunk

    def ffn_chunk(i, carry):
        ffn_cols(pl.ds(pl.multiple_of(i * chunk, chunk), chunk))
        return carry

    lax.fori_loop(0, full, ffn_chunk, 0)
    if ff % chunk:
        ffn_cols(pl.ds(full * chunk, ff % chunk))

    def down(who):
        at = pl.ds(pl.multiple_of(who * cols, cols), cols)
        part[:, at] = jnp.dot(
            hidden[...], s_all[who], preferred_element_type=f32
        ).astype(bf16)

    def down_copy(t, who):
        at = pl.ds(pl.multiple_of(who * cols, cols), cols)
        return remote(
            part.at[rows_of(t), at],
            recv2.at[block_of, :, at],
            t3_send.at[t, who],
            t3_recv.at[block_of, who],
            dev(pair0 + c, x, t // 2, t % 2),
        )

    def down_step(who):
        down(who)
        for t in range(n_tp):

            @pl.when(jnp.logical_or(c != b, mt != t))
            def _(t=t):
                down_copy(t, who).start()

        at = pl.ds(pl.multiple_of(who * cols, cols), cols)

        @pl.when(c == b)
        def _():
            recv2[block_of, :, at] = part[rows_of(mt), at]

    near_copy(0).wait_send()
    near_copy(1).wait_send()
    own_block([4, 5])
    down_step(me)
    relay_col(4)
    for us in ([4, 5],):
        for u in us:
            relay_x(u, [0])
        other_half(us, z * FAN + 1 - x)
    down_step(z * FAN + 1 - x)
    relay_col(5)
    for i in range(1, planes):
        who = plane_at(i) * FAN + x
        other_half([4, 5], who)
        down_step(who)
        relay_x(4, [i])
    for i in range(1, planes):
        who = plane_at(i) * FAN + 1 - x
        relay_x(5, [i])
        other_half([4, 5], who)
        down_step(who)

    def settle(who, carry):
        at = pl.ds(pl.multiple_of(who * cols, cols), cols)
        for t in range(n_tp):

            @pl.when(jnp.logical_or(c != b, block_of != t))
            def _(t=t):
                remote(
                    part.at[rows_of(t), at],
                    recv2.at[t, :, at],
                    t3_send.at[t, who],
                    t3_recv.at[t, who],
                    dev(z, x, y, 1 - c),
                ).wait_recv()

        return carry

    lax.fori_loop(0, n_sp, settle, 0)
    channel = recv2[0].astype(f32)
    for t in range(1, n_tp):
        channel = channel + recv2[t].astype(f32)
    out_ref[...] = layer_norm(
        ALPHA * own_norm[...].astype(f32) + channel, g2_ref[...]
    ).astype(bf16)

    def drain(who, carry):
        for t in range(n_tp):

            @pl.when(jnp.logical_or(c != b, mt != t))
            def _(t=t):
                down_copy(t, who).wait_send()

        @pl.when(who != me)
        def _():
            for u in range(len(units)):
                dr_copy(u, who).wait_send()

        return carry

    lax.fori_loop(0, n_sp, drain, 0)
    for u in range(len(units)):
        for i in range(1, planes):
            xr_copy(u, i).wait_send()
        for q in range(2):
            for j in range(dests):

                @pl.when(2 * j + c != z)
                def _(u=u, q=q, j=j):
                    z_copy(u, q, j).wait_send()

    @pl.when(c == b)
    def _():
        for u in range(len(units)):
            for q in range(2):
                xo_copy(u, q).wait_send()
                do_copy(u, q).wait_send()

    for copy in rim_copies:
        copy.wait_send()
    for k in range(strips):
        side_copy(k).wait_send()
        copies = ag_copies(k)
        copies[0].wait_send()
        copies[1].wait_send()

        @pl.when(c != b)
        def _(k=k, copies=copies):
            copies[2].wait_send()
            for pc in range(2):
                passed_on(pc, k).wait_send()

    @pl.when(tail)
    def _():
        for copy in halo_copies:
            copy.wait_send()

    for copy in state_copies(0):
        copy.wait_send()
    for d in range(1, half):

        @pl.when(me + 2 * d < n_sp)
        def _(d=d):
            for copy in state_copies(d):
                copy.wait_send()


def fused_shards(n_sp, n_tp, *args):
    (
        res, rv, xf, bf, cf, dt, doff, fade, elf, byp, xk, bk, ck, csv, mm, g1, v, w, s, vk, wk, g2
    ) = args
    f32, bf16 = jnp.float32, jnp.bfloat16
    rows, inner = xf.shape
    heads = dt.shape[1]
    width = mm.shape[1]
    ff = v.shape[1]
    own_rows = rows // n_tp
    row = lambda a: a.reshape(1, -1)
    half = n_sp // 2
    planes = n_sp // FAN
    units = 3 * HALVES
    vmem = pl.BlockSpec(memory_space=pltpu.VMEM)
    hbm = pl.BlockSpec(memory_space=pl.ANY)
    dma = pltpu.SemaphoreType.DMA
    return pl.pallas_call(
        functools.partial(layer_kernel, n_sp, n_tp),
        out_shape=jax.ShapeDtypeStruct(res.shape, bf16),
        in_specs=[hbm] * 2 + [vmem] * 12 + [hbm, vmem] + [hbm] * 3 + [vmem] * 3,
        out_specs=vmem,
        scratch_shapes=[
            pltpu.VMEM((n_sp * v.shape[0], ff), bf16),
            pltpu.VMEM((n_sp * v.shape[0], ff), bf16),
            pltpu.VMEM((n_sp,) + s.shape, bf16),
            pltpu.VMEM((RIM, inner), bf16),
            pltpu.VMEM((RIM, STATE), bf16),
            pltpu.VMEM((RIM, STATE), bf16),
            pltpu.VMEM(vk.shape, bf16),
            pltpu.VMEM(wk.shape, bf16),
            pltpu.VMEM((rows + RIM, 128), f32),
            pltpu.VMEM((rows, inner), bf16),
            pltpu.VMEM((rows, STATE), bf16),
            pltpu.VMEM((rows, STATE), bf16),
            pltpu.VMEM((heads, rows), f32),
            pltpu.VMEM((heads, rows), f32),
            pltpu.VMEM((rows, inner), f32),
            pltpu.VMEM((rows, heads), f32),
            pltpu.VMEM((8, heads), f32),
            pltpu.VMEM((STATE, inner), f32),
            pltpu.VMEM((STATE, inner), bf16),
            pltpu.VMEM((8, heads), f32),
            pltpu.VMEM((STATE, inner), bf16),
            pltpu.VMEM((8, heads), f32),
            pltpu.VMEM((half, STATE, inner), bf16),
            pltpu.VMEM((half, 8, heads), f32),
            pltpu.VMEM((rows, width), bf16),
            pltpu.VMEM((2, own_rows, width), bf16),
            pltpu.VMEM((own_rows, width), bf16),
            pltpu.VMEM((own_rows, width), bf16),
            pltpu.VMEM((own_rows, width), bf16),
            pltpu.VMEM((n_tp, own_rows, width), bf16),
            pltpu.VMEM((rows + RIM, width), bf16),
            pltpu.VMEM((rows, ff), bf16),
            pltpu.VMEM(res.shape, bf16),
            pltpu.VMEM(rv.shape, bf16),
            pltpu.VMEM(mm.shape, bf16),
            dma((3,)),
            dma((3,)),
            dma((units, 2, n_sp)),
            dma((units, 2, planes // 2)),
            dma((units, 2)),
            dma((units, 2)),
            dma((units, planes)),
            dma((units, n_sp)),
            dma((3,)),
            dma((3,)),
            dma((2,)),
            dma((2,)),
            dma((half, 2)),
            dma((half, 2)),
            dma((2,)),
            dma((2,)),
            dma((2,)),
            dma((2,)),
            dma((3, 2)),
            dma((n_tp, 2)),
            dma((2, 2)),
            dma((4,)),
            dma,
            dma((n_tp, n_sp)),
            dma((n_tp, n_sp)),
        ],
        compiler_params=pltpu.CompilerParams(
            collective_id=0, has_side_effects=True, vmem_limit_bytes=60 * 1024 * 1024
        ),
    )(
        res, rv, xf, bf, cf, dt.T, row(doff), row(fade), elf.T, row(byp), xk, bk, ck, row(csv), mm,
        row(g1), v, w, s, vk, wk, row(g2),
    )


def shards_for(n_sp, n_tp):
    def shards(*args):
        rows = args[2].shape[0]
        fits = (
            args[3].shape[1] == STATE
            and args[18].shape[1] % 128 == 0
            and args[16].shape[0] % 64 == 0
            and args[16].shape[1] % 128 == 0
            and n_sp % (2 * FAN) == 0
            and n_sp > 2 * FAN
            and n_tp == 4
            and args[18].shape[0] % 64 == 0
            and rows % (BLOCK * n_tp) == 0
        )
        if fits:
            return fused_shards(n_sp, n_tp, *args)
        return plain_shards(*args)

    return shards


def solution(mesh):
    in_specs = (
        P(("sp", "tp"), None),
        P("sp", "tp"),
        P("sp", "tp"),
        P("sp", "tp"),
        P("sp", "tp"),
        P("sp", "tp"),
        P("tp"),
        P("tp"),
        P("sp", "tp"),
        P("tp"),
        P(None, "tp"),
        P(None, "tp"),
        P(None, "tp"),
        P("tp"),
        P("tp", None),
        P(),
        P("sp", "tp"),
        P("sp", "tp"),
        P("tp", "sp"),
        P(None, "tp"),
        P(None, "tp"),
        P(),
    )
    out_specs = P(("sp", "tp"), None)
    shards = shards_for(mesh.shape["sp"], mesh.shape["tp"])
    return jax.shard_map(shards, mesh=mesh, in_specs=in_specs, out_specs=out_specs, check_vma=False)
```

```python
import functools
import jax
import jax.numpy as jnp
from jax import lax
from jax.experimental import pallas as pl
from jax.experimental.pallas import tpu as pltpu
from jax.sharding import PartitionSpec as P

HEADS = 32
HEAD_DIM = 64
GROUPS = 4
STATE = 128
CONV = 4
FCONV = 3
BLOCK = 128


EPSILON = 1e-05
ALPHA = 2.0**0.25
HIGHEST = lax.Precision.HIGHEST


def shifted(shard, axis, by):
    count = lax.axis_size(axis)
    pairs = [(i, i + by) for i in range(count) if 0 <= i + by < count]
    return lax.ppermute(shard, axis, pairs)


def entering(shard, axis, join, neutral):
    place = lax.axis_index(axis)
    gathered = jax.tree.map(
        lambda a, kind: lax.all_gather(a.astype(kind), axis), shard, (jnp.bfloat16, jnp.bfloat16)
    )
    state = jax.tree.map(lambda a, e: jnp.zeros_like(a) + jnp.asarray(e, a.dtype), shard, neutral)

    def one(lap, state):
        return join(
            state,
            jax.tree.map(
                lambda a, own: lax.dynamic_index_in_dim(a, lap, 0, False).astype(own.dtype),
                gathered,
                shard,
            ),
        )

    return lax.fori_loop(0, place, one, state)


def causal_conv(signal, before, tap_weights):
    tap_count = tap_weights.shape[0]
    row_count = signal.shape[0]
    padded = jnp.concatenate([before, signal], axis=0).astype(jnp.float32)
    running = jnp.zeros(signal.shape, jnp.float32)
    for tap_index in range(tap_count):
        running = (
            running
            + tap_weights[tap_index].astype(jnp.float32) * padded[tap_index : tap_index + row_count]
        )
    return running


def layer_norm(values, scales):
    row_mean = jnp.mean(values, axis=-1, keepdims=True)
    centred = values - row_mean
    spread = jnp.mean(centred * centred, axis=-1, keepdims=True)
    return centred * lax.rsqrt(spread + EPSILON) * scales


def combine_states(earlier_pair, later_pair):
    return (
        earlier_pair[0] * later_pair[1][..., None, None] + later_pair[0],
        earlier_pair[1] * later_pair[1],
    )


def chain_step(state_now, inputs):
    fresh_one, decay_one = inputs
    return (state_now * decay_one[..., None, None] + fresh_one, state_now)


def plain_shards(
    incoming_residual_stream,
    result_valve,
    channel_feed_matrix,
    memory_feed_matrix,
    memory_query_matrix,
    unsoftened_deltas,
    delta_offset,
    channel_fading_speed,
    extra_log_fading,
    bypass_factor,
    channel_feed_kernel,
    memory_feed_kernel,
    memory_query_kernel,
    cluster_scaling_vector,
    mixer_result_matrix,
    initial_scaling_vector,
    valve_matrix,
    widen_matrix,
    shrink_matrix,
    valve_filter_kernel,
    widen_filter_kernel,
    latter_scaling_vector,
):
    row_count = channel_feed_matrix.shape[0]
    inner_here = channel_feed_matrix.shape[1]
    group_count = memory_feed_matrix.shape[1] // STATE
    group_heads = HEADS // GROUPS
    block_count = row_count // BLOCK
    rim_rows = CONV - 1
    rim_x, rim_b, rim_c = shifted(
        (
            channel_feed_matrix[row_count - rim_rows :],
            memory_feed_matrix[row_count - rim_rows :],
            memory_query_matrix[row_count - rim_rows :],
        ),
        "sp",
        1,
    )
    x_act = jax.nn.silu(causal_conv(channel_feed_matrix, rim_x, channel_feed_kernel)).astype(
        jnp.bfloat16
    )
    b_act = jax.nn.silu(causal_conv(memory_feed_matrix, rim_b, memory_feed_kernel)).astype(
        jnp.bfloat16
    )
    c_act = jax.nn.silu(causal_conv(memory_query_matrix, rim_c, memory_query_kernel)).astype(
        jnp.bfloat16
    )
    channel_delta_amount = jax.nn.softplus(unsoftened_deltas + delta_offset[None, :])
    log_fading_amount = extra_log_fading - channel_fading_speed[None, :] * channel_delta_amount
    x_heads = x_act.astype(jnp.float32).reshape(row_count, group_count, group_heads, HEAD_DIM)
    x_scaled = (
        x_heads * channel_delta_amount.reshape(row_count, group_count, group_heads)[..., None]
    )
    b_full = b_act.astype(jnp.float32).reshape(row_count, group_count, STATE)
    c_full = c_act.astype(jnp.float32).reshape(row_count, group_count, STATE)
    decay_full = log_fading_amount.reshape(row_count, group_count, group_heads)
    x_blk = x_scaled.reshape(block_count, BLOCK, group_count, group_heads, HEAD_DIM)
    b_blk = b_full.reshape(block_count, BLOCK, group_count, STATE)
    c_blk = c_full.reshape(block_count, BLOCK, group_count, STATE)
    b_narrow = b_act.reshape(block_count, BLOCK, group_count, STATE)
    c_narrow = c_act.reshape(block_count, BLOCK, group_count, STATE)
    decay_blk = decay_full.reshape(block_count, BLOCK, group_count, group_heads)
    cum_decay = jnp.cumsum(decay_blk, axis=1)
    causal = jnp.tril(jnp.ones((BLOCK, BLOCK), dtype=bool))
    between = cum_decay[:, :, None] - cum_decay[:, None, :]
    lag = jnp.exp(jnp.where(causal[None, :, :, None, None], between, -jnp.inf))
    affinity = jnp.einsum("blgn,bsgn->blsg", c_narrow, b_narrow, preferred_element_type=jnp.float32)
    mixing = affinity[..., None] * lag
    within = jnp.einsum("blsgh,bsghp->blghp", mixing, x_blk, precision=HIGHEST)
    to_end = jnp.exp(cum_decay[:, -1:] - cum_decay)
    fresh = jnp.einsum("blgn,blghp->bghpn", b_blk, x_blk * to_end[..., None], precision=HIGHEST)
    block_decay = jnp.exp(cum_decay[:, -1])
    initial = jnp.zeros((group_count, group_heads, HEAD_DIM, STATE), jnp.float32)
    local_end, earlier = lax.scan(chain_step, initial, (fresh, block_decay))
    carried = (
        jnp.einsum("blgn,bghpn->blghp", c_blk, earlier, precision=HIGHEST)
        * jnp.exp(cum_decay)[..., None]
    )
    from_start = jnp.cumsum(decay_full, axis=0)
    incoming, _ = entering(
        (local_end, jnp.exp(from_start[-1])),
        "sp",
        combine_states,
        (jnp.zeros_like(local_end), jnp.ones_like(from_start[-1])),
    )
    arriving = (
        jnp.einsum("tgn,ghpn->tghp", c_full, incoming, precision=HIGHEST)
        * jnp.exp(from_start)[..., None]
    )
    y_heads = (within + carried).reshape(row_count, group_count, group_heads, HEAD_DIM) + arriving
    y_heads = y_heads + bypass_factor.reshape(group_count, group_heads)[None, :, :, None] * x_heads
    gated = y_heads.reshape(row_count, group_count, group_heads * HEAD_DIM)
    gated = gated * jax.nn.silu(result_valve.astype(jnp.float32)).reshape(
        row_count, group_count, group_heads * HEAD_DIM
    )
    gated = gated * lax.rsqrt(jnp.mean(gated * gated, axis=-1, keepdims=True) + EPSILON)
    y_norm = (gated.reshape(row_count, inner_here) * cluster_scaling_vector[None, :]).astype(
        jnp.bfloat16
    )
    mixer = lax.psum_scatter(
        jnp.dot(y_norm, mixer_result_matrix, preferred_element_type=jnp.float32).astype(
            jnp.bfloat16
        ),
        "tp",
        scatter_dimension=0,
        tiled=True,
    ).astype(jnp.float32)
    normed_own = layer_norm(
        ALPHA * incoming_residual_stream.astype(jnp.float32) + mixer, initial_scaling_vector
    ).astype(jnp.bfloat16)
    normed_all = lax.all_gather(normed_own, "tp", axis=0, tiled=True)
    gate_sum = jnp.dot(
        normed_all,
        lax.all_gather(valve_matrix, "sp", axis=0, tiled=True),
        preferred_element_type=jnp.float32,
    )
    up_sum = jnp.dot(
        normed_all,
        lax.all_gather(widen_matrix, "sp", axis=0, tiled=True),
        preferred_element_type=jnp.float32,
    )
    gate_proj = gate_sum.astype(jnp.bfloat16)
    up_proj = up_sum.astype(jnp.bfloat16)
    ffn_rows = FCONV - 1
    rim_gate, rim_up = shifted(
        (gate_proj[row_count - ffn_rows :], up_proj[row_count - ffn_rows :]), "sp", 1
    )
    gate_conv = causal_conv(gate_proj, rim_gate, valve_filter_kernel)
    up_conv = causal_conv(up_proj, rim_up, widen_filter_kernel)
    hidden = (jax.nn.silu(gate_conv) * up_conv).astype(jnp.bfloat16)
    channel_part = jnp.dot(
        hidden,
        lax.all_gather(shrink_matrix, "sp", axis=1, tiled=True),
        preferred_element_type=jnp.float32,
    )
    channel = lax.psum_scatter(
        channel_part.astype(jnp.bfloat16), "tp", scatter_dimension=0, tiled=True
    ).astype(jnp.float32)
    return layer_norm(
        ALPHA * normed_own.astype(jnp.float32) + channel, latter_scaling_vector
    ).astype(jnp.bfloat16)


MESH = pl.DeviceIdType.MESH
RIM = 16
FAN = 2
CUTS = (2, 2, 4)


def silu(v):
    return v / (1.0 + jnp.exp(-v))


def layer_kernel(
    n_sp,
    n_tp,
    res_hbm,
    rv_hbm,
    xf_ref,
    bf_ref,
    cf_ref,
    dt_ref,
    doff_ref,
    fade_ref,
    elf_ref,
    byp_ref,
    xk_ref,
    bk_ref,
    ck_ref,
    csv_ref,
    mm_hbm,
    g1_ref,
    v_hbm,
    w_hbm,
    s_hbm,
    vk_ref,
    wk_ref,
    g2_ref,
    out_ref,
    v_all,
    w_all,
    s_all,
    rim_x,
    rim_b,
    rim_c,
    vk_other,
    wk_other,
    ext,
    x_act,
    b_act,
    c_act,
    step_ref,
    ld_ref,
    y_ref,
    efs_ref,
    base_ref,
    state_ref,
    st_send,
    dec_send,
    pair_send,
    pair_dec,
    st_recv,
    dec_recv,
    part,
    near_recv,
    side_send,
    side_recv,
    own_norm,
    recv2,
    pre_recv,
    normed,
    hidden,
    res_ref,
    rv_ref,
    mm_ref,
    late_sem,
    own_sem,
    w_recv,
    z_send,
    xo_send,
    do_send,
    xr_send,
    dr_send,
    rim_send,
    rim_recv,
    tap_send,
    tap_recv,
    st_ssem,
    st_rsem,
    a_send,
    a_recv,
    b_send,
    b_recv,
    ag_send,
    ag_recv,
    agr_send,
    halo_send,
    halo_recv,
    t3_send,
    t3_recv,
    p_send,
    p_recv,
):
    f32, bf16 = jnp.float32, jnp.bfloat16
    rows, inner = xf_ref.shape
    heads = dt_ref.shape[0]
    own_rows = rows // n_tp
    width = mm_hbm.shape[1]
    ff = v_hbm.shape[1]
    depth = v_hbm.shape[0]
    cols = s_hbm.shape[1]
    blocks = rows // BLOCK
    planes = n_sp // FAN
    dests = planes // 2
    half = n_sp // 2
    me = lax.axis_index("sp")
    mt = lax.axis_index("tp")
    z, x = me // FAN, me % FAN
    y, c = mt // 2, mt % 2
    b = z % 2
    mate = z + 1 - 2 * b
    pair0 = z - b

    def dev(pz, px, py, pc):
        return (pz * FAN + px, py * 2 + pc)

    def remote(src, dst, send, recv, device):
        return pltpu.make_async_remote_copy(
            src_ref=src, dst_ref=dst, send_sem=send, recv_sem=recv, device_id=device, device_id_type=MESH
        )

    barrier = pltpu.get_barrier_semaphore()
    total_devices = n_sp * n_tp
    line = me * n_tp + mt
    for d in range(1, total_devices):
        who = (line + d) % total_devices
        pl.semaphore_signal(barrier, inc=1, device_id=(who // n_tp, who % n_tp), device_id_type=MESH)
    pl.semaphore_wait(barrier, total_devices - 1)

    units = [(kind, g) for kind in range(3) for g in range(CUTS[kind])]
    sources = (v_hbm, w_hbm, s_hbm)

    def place(u, q):
        kind, g = units[u]
        size = (ff if kind == 2 else depth) // (2 * CUTS[kind])
        return size, (q * CUTS[kind] + g) * size

    def own_piece(u, q):
        size, at = place(u, q)
        return sources[units[u][0]].at[pl.ds(pl.multiple_of(at, 16), size)]

    def slot(u, q, who):
        size, at = place(u, q)
        kind = units[u][0]
        if kind == 2:
            return s_all.at[who, pl.ds(pl.multiple_of(at, 16), size)]
        whole = v_all if kind == 0 else w_all
        return whole.at[pl.ds(pl.multiple_of(who * depth + at, 16), size)]

    def landed(u, q, who):
        here = slot(u, q, who)
        return remote(here, here, do_send.at[0, 0], w_recv.at[u, q, who], dev(z, x, y, 1 - c))

    def z_copy(u, q, j):
        return remote(
            own_piece(u, q),
            slot(u, q, me),
            z_send.at[u, q, j],
            w_recv.at[u, q, me],
            dev(2 * j + c, x, y, q),
        )

    def xo_copy(u, q):
        return remote(
            own_piece(u, q), slot(u, q, me), xo_send.at[u, q], w_recv.at[u, q, me], dev(z, 1 - x, y, q)
        )

    def do_copy(u, q):
        return remote(
            own_piece(u, q), slot(u, q, me), do_send.at[u, q], w_recv.at[u, q, me], dev(z, x, y, 1 - c)
        )

    def xr_copy(u, i):
        here = slot(u, c, plane_at(i) * FAN + x)
        return remote(
            here,
            here,
            xr_send.at[u, i],
            w_recv.at[u, c, plane_at(i) * FAN + x],
            dev(z, 1 - x, y, c),
        )

    def dr_copy(u, who):
        here = slot(u, c, who)
        return remote(here, here, dr_send.at[u, who], w_recv.at[u, c, who], dev(z, x, y, 1 - c))

    def plane_at(i):
        if i == 0:
            return z
        low = jnp.where(z < planes // 2, z, planes - 1 - z)
        got = jnp.where(i - 1 < low, i - 1, i)
        return jnp.where(z < planes // 2, got, planes - 1 - got)

    def send_z(pieces, only=True):
        for u, q in pieces:
            for j in range(dests):

                @pl.when(jnp.logical_and(2 * j + c != z, only if only is True else only(2 * j + c)))
                def _(u=u, q=q, j=j):
                    z_copy(u, q, j).start()

    def both(us):
        return [(u, q) for u in us for q in range(2)]

    def held(to):
        return jnp.logical_and(jnp.logical_and(b == 0, to > z), z < planes - 2)

    def free(to):
        return jnp.logical_not(held(to))

    def send_xo(which):
        @pl.when(c == b)
        def _():
            for u in which:
                for q in range(2):
                    xo_copy(u, q).start()

    def relay_col(u, picks=None):
        for i in picks or range(1, planes):
            who = plane_at(i) * FAN + x
            landed(u, c, who).wait_recv()
            xr_copy(u, i).start()
            dr_copy(u, who).start()

    def relay_x(u, picks=None):
        for i in picks or range(planes):
            who = plane_at(i) * FAN + 1 - x
            landed(u, c, who).wait_recv()
            dr_copy(u, who).start()

    def other_half(us, who):
        for u in us:
            landed(u, 1 - c, who).wait_recv()

    def own_block(us):
        @pl.when(c != b)
        def _():
            for u in us:
                for q in range(2):
                    landed(u, q, me).wait_recv()

    rim_copies = []
    for i, (src, dst) in enumerate(((xf_ref, rim_x), (bf_ref, rim_b), (cf_ref, rim_c))):
        rim_copies.append(
            remote(
                src.at[pl.ds(rows - RIM, RIM)],
                dst,
                rim_send.at[i],
                rim_recv.at[i],
                ((me + 1) % n_sp, mt),
            )
        )
        rim_copies[-1].start()
    tap_copies = [
        remote(src, dst, tap_send.at[i], tap_recv.at[i], dev(z, x, y, 1 - c))
        for i, (src, dst) in enumerate(((vk_ref, vk_other), (wk_ref, wk_other)))
    ]
    for copy in tap_copies:
        copy.start()
    send_z(both([0]))
    send_xo([0, 1])

    own_copies = []
    for kind in range(3):
        dst = s_all.at[me] if kind == 2 else (v_all, w_all)[kind].at[
            pl.ds(pl.multiple_of(me * depth, 16), depth)
        ]
        own_copies.append(pltpu.make_async_copy(sources[kind], dst, own_sem.at[kind]))

    @pl.when(c == b)
    def _():
        for u in range(len(units)):
            for q in range(2):
                do_copy(u, q).start()
        for copy in own_copies:
            copy.start()

    late = [
        pltpu.make_async_copy(src, dst, late_sem.at[i])
        for i, (src, dst) in enumerate(((rv_hbm, rv_ref), (mm_hbm, mm_ref), (res_hbm, res_ref)))
    ]
    for copy in late:
        copy.start()

    eye = lax.broadcasted_iota(jnp.int32, (heads, heads), 0) == lax.broadcasted_iota(
        jnp.int32, (heads, heads), 1
    )

    def column(a):
        return jnp.sum(jnp.where(eye, a[...], 0.0), axis=1, keepdims=True)

    raw = dt_ref[...] + column(doff_ref)
    step_ref[...] = jnp.maximum(raw, 0.0) + jnp.log1p(jnp.exp(-jnp.abs(raw)))
    ld_ref[...] = elf_ref[...] - column(fade_ref) * step_ref[...]

    for copy in rim_copies:
        copy.wait_recv()
    first = me == 0
    for rim, feed, taps, act in (
        (rim_x, xf_ref, xk_ref, x_act),
        (rim_b, bf_ref, bk_ref, b_act),
        (rim_c, cf_ref, ck_ref, c_act),
    ):
        for lo in range(0, feed.shape[1], 128):
            here = slice(lo, lo + 128)
            edge = rim[:, here].astype(f32)
            ext[0:RIM, :] = jnp.where(first, jnp.zeros_like(edge), edge)
            ext[RIM:, :] = feed[:, here].astype(f32)
            tap = taps[:, here].astype(f32)
            total = jnp.zeros((rows, 128), f32)
            for k in range(CONV):
                start = RIM - (CONV - 1) + k
                total = total + tap[k : k + 1] * ext[start : start + rows, :]
            act[:, here] = silu(total).astype(bf16)

    li = lax.broadcasted_iota(jnp.int32, (BLOCK, BLOCK), 0)
    si = lax.broadcasted_iota(jnp.int32, (BLOCK, BLOCK), 1)
    causal = li >= si
    lower = jnp.where(causal, 1.0, 0.0).astype(f32)
    upper = jnp.where(li <= si, 1.0, 0.0).astype(f32)
    spread = jnp.where(
        lax.broadcasted_iota(jnp.int32, (heads, inner), 1) // HEAD_DIM
        == lax.broadcasted_iota(jnp.int32, (heads, inner), 0),
        1.0,
        0.0,
    ).astype(f32)
    near = lax.broadcasted_iota(jnp.int32, (BLOCK, 2 * HEAD_DIM), 1) < HEAD_DIM

    def widen(a):
        return jnp.dot(a, spread, precision=HIGHEST, preferred_element_type=f32)

    state_ref[...] = jnp.zeros_like(state_ref)
    base_ref[...] = jnp.zeros_like(base_ref)
    skip = widen(byp_ref[...])

    def scan_block(i, carry):
        at = pl.ds(pl.multiple_of(i * BLOCK, BLOCK), BLOCK)
        ld = ld_ref[:, at]
        cum = lax.dot_general(
            lower, ld, (((1,), (1,)), ((), ())), precision=HIGHEST, preferred_element_type=f32
        )
        cum_t = jnp.dot(ld, upper, precision=HIGHEST, preferred_element_type=f32)
        last = cum[BLOCK - 1 : BLOCK, :]
        xx = x_act[at, :].astype(f32)
        bb = b_act[at, :]
        cc = c_act[at, :]
        xs = xx * lax.dot_general(
            step_ref[:, at],
            spread,
            (((0,), (0,)), ((), ())),
            precision=HIGHEST,
            preferred_element_type=f32,
        )
        xs16 = xs.astype(bf16)
        aff = lax.dot_general(
            cc, bb, (((1,), (1,)), ((), ())), preferred_element_type=f32
        )
        yy = (
            jnp.dot(cc, state_ref[...].astype(bf16), preferred_element_type=f32)
            * widen(jnp.exp(cum))
            + skip * xx
        )
        for pair in range(heads // 2):
            at_pair = slice(pair * 2 * HEAD_DIM, (pair + 1) * 2 * HEAD_DIM)
            both = []
            for h in (2 * pair, 2 * pair + 1):
                gap = cum[:, h : h + 1] - cum_t[h : h + 1, :]
                lag = jnp.exp(jnp.where(causal, gap, -1e30))
                both.append(
                    jnp.dot(
                        (aff * lag).astype(bf16), xs16[:, at_pair], preferred_element_type=f32
                    )
                )
            y_ref[at, at_pair] = yy[:, at_pair] + jnp.where(near, both[0], both[1])
        fresh = lax.dot_general(
            bb,
            (xs * widen(jnp.exp(last - cum))).astype(bf16),
            (((0,), (0,)), ((), ())),
            preferred_element_type=f32,
        )
        state_ref[...] = state_ref[...] * widen(jnp.exp(last)) + fresh
        base = base_ref[0:1, :]
        efs_ref[at, :] = jnp.exp(base + cum)
        base_ref[0:1, :] = base + last
        return carry

    lax.fori_loop(0, blocks, scan_block, 0)
    st_send[...] = state_ref[...].astype(bf16)
    dec_send[...] = jnp.broadcast_to(base_ref[0:1, :], dec_send.shape)
    odd = me % 2
    partner = me + 1 - 2 * odd

    pairs = planes // 2
    own_pair = z // 2

    def state_copy(src, src_dec, at, sent, device):
        return [
            remote(a, o.at[at], st_ssem.at[sent, i], st_rsem.at[at, i], device)
            for i, (a, o) in enumerate(((src, st_recv), (src_dec, dec_recv)))
        ]

    beside_copies = state_copy(st_send, dec_send, 0, 0, (partner, mt))
    mate_copies = state_copy(pair_send, pair_dec, 1, 1, dev(mate, x, y, c))

    def quad_copies(j, side):
        to = jnp.minimum(2 * j + side, planes - 1)
        return state_copy(pair_send, pair_dec, 2 + own_pair, 2 + 2 * j + side, dev(to, x, y, c))

    for copy in beside_copies:
        copy.start()
    for copy in beside_copies:
        copy.wait_recv()
    own_dec = widen(jnp.exp(dec_send[0:1, :]))
    beside_dec = widen(jnp.exp(dec_recv[0, 0:1, :]))
    beside = st_recv[0].astype(f32)
    later = odd == 1
    plane_state = jnp.where(
        later, state_ref[...] + beside * own_dec, state_ref[...] * beside_dec + beside
    )

    @pl.when(b == 0)
    def _():
        pair_send[...] = plane_state.astype(bf16)
        pair_dec[...] = dec_send[...] + dec_recv[0]
        for copy in mate_copies:
            copy.start()

    @pl.when(b == 1)
    def _():
        for copy in mate_copies:
            copy.wait_recv()
        plane_dec = dec_send[...] + dec_recv[0]
        pair_send[...] = (
            st_recv[1].astype(f32) * widen(jnp.exp(plane_dec[0:1, :])) + plane_state
        ).astype(bf16)
        pair_dec[...] = plane_dec + dec_recv[1]
        for j in range(1, pairs):
            for side in (1, 0):

                @pl.when(own_pair < j)
                def _(j=j, side=side):
                    for copy in quad_copies(j, side):
                        copy.start()

    state_ref[...] = jnp.zeros_like(state_ref)
    send_z(both([1, 2]), free)
    send_xo(range(2, len(units)))

    def join(at):
        state_ref[...] = state_ref[...] * widen(jnp.exp(dec_recv[at, 0:1, :])) + st_recv[at].astype(f32)

    for j in range(pairs - 1):

        @pl.when(own_pair > j)
        def _(j=j):
            for copy in state_copy(pair_send, pair_dec, 2 + j, 0, dev(mate, x, y, c)):
                copy.wait_recv()
            join(2 + j)

    @pl.when(b == 1)
    def _():
        join(1)

    @pl.when(odd == 1)
    def _():
        join(0)

    for copy in late:
        copy.wait()

    def project_block(i, carry):
        at = pl.ds(pl.multiple_of(i * BLOCK, BLOCK), BLOCK)
        yy = y_ref[at, :] + jnp.dot(
            c_act[at, :], state_ref[...].astype(bf16), preferred_element_type=f32
        ) * widen(efs_ref[at, :])
        gated = yy * silu(rv_ref[at, :].astype(f32))
        gated = gated * lax.rsqrt(jnp.mean(gated * gated, axis=-1, keepdims=True) + EPSILON)
        y_norm = (gated * csv_ref[...]).astype(bf16)
        part[at, :] = jnp.dot(y_norm, mm_ref[...], preferred_element_type=f32).astype(bf16)
        return carry

    def rows_of(t):
        return pl.ds(pl.multiple_of(t * own_rows, own_rows), own_rows)

    def near_copy(py):
        return remote(
            part.at[rows_of(py * 2 + 1 - c)],
            near_recv.at[py],
            a_send.at[py],
            a_recv.at[py],
            dev(z, x, y, 1 - c),
        )

    halfway = blocks // 2
    lax.fori_loop((1 - y) * halfway, (2 - y) * halfway, project_block, 0)
    near_copy(1 - y).start()
    lax.fori_loop(y * halfway, (y + 1) * halfway, project_block, 0)
    near_copy(y).start()

    strips = 2
    strip = own_rows // strips

    def side_copy(k):
        at = pl.ds(k * strip, strip)
        return remote(
            side_send.at[at], side_recv.at[at], b_send.at[k], b_recv.at[k], dev(z, x, 1 - y, c)
        )

    near_copy(1 - y).wait_recv()
    for k in range(strips):
        away = pl.ds(pl.multiple_of(((1 - y) * 2 + c) * own_rows + k * strip, strip), strip)
        side_send[k * strip : (k + 1) * strip, :] = (
            part[away, :].astype(f32) + near_recv[1 - y, k * strip : (k + 1) * strip, :].astype(f32)
        ).astype(bf16)
        side_copy(k).start()
    near_copy(y).wait_recv()
    relay_col(0)

    def ag_copies(k):
        lo = pl.ds(k * strip, strip)
        to = normed.at[pl.ds(pl.multiple_of(RIM + mt * own_rows + k * strip, RIM), strip)]
        return [
            remote(own_norm.at[lo], to, ag_send.at[i, k], ag_recv.at[mt, k], device)
            for i, device in enumerate((dev(mate, x, y, b), dev(z, x, 1 - y, b), dev(z, x, y, b)))
        ]

    for k in range(strips):
        side_copy(k).wait_recv()
        lo = slice(k * strip, (k + 1) * strip)
        mine = pl.ds(pl.multiple_of(mt * own_rows + k * strip, strip), strip)
        mixer = (
            part[mine, :].astype(f32)
            + near_recv[y, lo, :].astype(f32)
            + side_recv[lo, :].astype(f32)
        )
        own_norm[lo, :] = layer_norm(
            ALPHA * res_ref[lo, :].astype(f32) + mixer, g1_ref[...]
        ).astype(bf16)
        copies = ag_copies(k)
        copies[0].start()
        copies[1].start()

        @pl.when(c != b)
        def _(copies=copies):
            copies[2].start()

        @pl.when(c == b)
        def _(k=k, lo=lo):
            normed[pl.ds(pl.multiple_of(RIM + mt * own_rows + k * strip, RIM), strip), :] = own_norm[
                lo, :
            ]

    nxt = me + 1
    nz, nx = nxt // FAN, nxt % FAN
    tail = jnp.logical_and(mt == n_tp - 1, nxt < n_sp)
    halo_copies = [
        remote(
            own_norm.at[pl.ds(own_rows - RIM, RIM)],
            normed.at[pl.ds(0, RIM)],
            halo_send.at[i],
            halo_recv,
            dev(jnp.minimum(nz, planes - 1) // 2 * 2 + i // 2, nx, i % 2, nz % 2),
        )
        for i in range(4)
    ]

    @pl.when(tail)
    def _():
        for copy in halo_copies:
            copy.start()

    send_z(both([1, 2]), held)
    send_z(both([3]))
    outer = jnp.logical_or(z == 0, z == planes - 1)
    shrink = range(4, len(units))

    def far_outer(to):
        return jnp.logical_and(outer, jnp.abs(to - z) > 1)

    send_z(both(shrink), lambda to: jnp.logical_not(far_outer(to)))

    def gathered(t, k):
        here = normed.at[pl.ds(pl.multiple_of(RIM + t * own_rows + k * strip, RIM), strip)]
        return remote(here, here, ag_send.at[0, 0], ag_recv.at[t, k], dev(z, x, y, 1 - c))

    def passed_on(pc, k):
        here = normed.at[pl.ds(pl.multiple_of(RIM + (y * 2 + pc) * own_rows + k * strip, RIM), strip)]
        return remote(here, here, agr_send.at[pc, k], ag_recv.at[y * 2 + pc, k], dev(z, x, 1 - y, c))

    seg = (pair0 + c) * FAN + x

    relay_col(1)

    @pl.when(c != b)
    def _():
        for k in range(strips):
            for pc in range(2):
                gathered(y * 2 + pc, k).wait_recv()
                passed_on(pc, k).start()

    relay_col(2)
    relay_col(3)
    @pl.when(seg == 0)
    def _():
        normed[0:RIM, :] = jnp.zeros((RIM, width), bf16)

    @pl.when(seg > 0)
    def _():
        halo_copies[0].wait_recv()

    for k in range(strips):

        @pl.when(c == b)
        def _(k=k):
            gathered(y * 2 + 1 - c, k).wait_recv()

        for pc in range(2):
            gathered((1 - y) * 2 + pc, k).wait_recv()

    for u in range(4):
        relay_x(u)

    @pl.when(c == b)
    def _():
        for copy in own_copies:
            copy.wait()

    own_block(range(4))

    def rest(who, carry):
        @pl.when(who != me)
        def _():
            other_half(range(4), who)

        return carry

    lax.fori_loop(0, n_sp, rest, 0)
    for copy in tap_copies:
        copy.wait()
    send_z(both(shrink), lambda to: jnp.logical_and(far_outer(to), to < z))
    same = c == b

    def ffn_cols(at):
        feeds = normed[...]
        convs = []
        for weights, taps, others in ((v_all, vk_ref, vk_other), (w_all, wk_ref, wk_other)):
            proj = jnp.dot(feeds, weights[:, at], preferred_element_type=f32)
            proj = proj.astype(bf16).astype(f32)
            tap = jnp.where(same, taps[:, at].astype(f32), others[:, at].astype(f32))
            total = jnp.zeros((rows, proj.shape[1]), f32)
            for k in range(FCONV):
                start = RIM - (FCONV - 1) + k
                total = total + tap[k : k + 1] * proj[start : start + rows, :]
            convs.append(total)
        hidden[:, at] = (silu(convs[0]) * convs[1]).astype(bf16)

    chunk = 256
    full = ff // chunk

    def ffn_chunk(i, carry):
        ffn_cols(pl.ds(pl.multiple_of(i * chunk, chunk), chunk))
        return carry

    def relay_s(i):
        for u in shrink:
            relay_col(u, [i])

    relay_s(1)
    lax.fori_loop(0, full // 2, ffn_chunk, 0)
    relay_s(2)
    lax.fori_loop(full // 2, full // 2 + 1, ffn_chunk, 0)
    send_z(both(shrink), lambda to: jnp.logical_and(far_outer(to), to > z))
    lax.fori_loop(full // 2 + 1, full, ffn_chunk, 0)
    if ff % chunk:
        ffn_cols(pl.ds(full * chunk, ff % chunk))

    def down(who):
        at = pl.ds(pl.multiple_of(who * cols, cols), cols)
        part[:, at] = jnp.dot(
            hidden[...], s_all[who], preferred_element_type=f32
        ).astype(bf16)

    def at_of(who):
        return pl.ds(pl.multiple_of(who * cols, cols), cols)

    def side_half(py):
        return pl.ds(pl.multiple_of(py * 2 * own_rows, own_rows), 2 * own_rows)

    def home_copies(who):
        at = at_of(who)
        return [
            remote(
                part.at[rows_of(py * 2 + pc), at],
                recv2.at[y, :, at],
                t3_send.at[i, who],
                t3_recv.at[y, who],
                dev(z, x, py, pc),
            )
            for i, (py, pc) in enumerate(((1 - y, 0), (1 - y, 1), (y, 1 - c)))
        ]

    def cross_copy(who):
        at = at_of(who)
        return remote(
            part.at[side_half(1 - y), at], pre_recv.at[:, at], p_send.at[who], p_recv.at[who], dev(z, x, 1 - y, c)
        )

    def away_copies(who):
        at = at_of(who)
        return [
            remote(
                part.at[rows_of(y * 2 + pc), at],
                recv2.at[2, :, at],
                t3_send.at[pc, who],
                t3_recv.at[2, who],
                dev(mate, x, y, pc),
            )
            for pc in range(2)
        ]

    done = []
    lag = 2

    def finish(who):
        at = at_of(who)

        @pl.when(c != b)
        def _():
            cross_copy(who).wait_recv()
            here = side_half(y)
            part[here, at] = (part[here, at].astype(f32) + pre_recv[:, at].astype(f32)).astype(bf16)
            for copy in away_copies(who):
                copy.start()

    def down_step(who):
        down(who)
        at = at_of(who)

        @pl.when(c != b)
        def _():
            cross_copy(who).start()

        @pl.when(c == b)
        def _():
            for copy in home_copies(who):
                copy.start()
            recv2[y, :, at] = part[rows_of(mt), at]

        done.append(who)
        if len(done) > lag:
            finish(done[-1 - lag])

    near_copy(0).wait_send()
    near_copy(1).wait_send()
    own_block(shrink)
    down_step(me)

    def x_step(i):
        who = plane_at(i) * FAN + 1 - x
        for u in shrink:
            relay_x(u, [i])
        other_half(shrink, who)
        down_step(who)

    def col_step(i):
        who = plane_at(i) * FAN + x
        other_half(shrink, who)
        down_step(who)

    x_step(0)
    col_step(1)
    x_step(1)
    for i in range(2, planes - 1):
        col_step(i)
        for u in shrink:
            relay_col(u, [i + 1])
        x_step(i)
    col_step(planes - 1)
    x_step(planes - 1)
    for who in done[-lag:]:
        finish(who)

    def settle(who, carry):
        at = at_of(who)
        for t in range(3):

            @pl.when(jnp.logical_or(c != b, y != t))
            def _(t=t):
                remote(
                    part.at[rows_of(t), at],
                    recv2.at[t, :, at],
                    t3_send.at[t, who],
                    t3_recv.at[t, who],
                    dev(z, x, y, 1 - c),
                ).wait_recv()

        return carry

    lax.fori_loop(0, n_sp, settle, 0)
    channel = recv2[0].astype(f32)
    for t in range(1, 3):
        channel = channel + recv2[t].astype(f32)
    out_ref[...] = layer_norm(
        ALPHA * own_norm[...].astype(f32) + channel, g2_ref[...]
    ).astype(bf16)

    def drain(who, carry):
        @pl.when(c == b)
        def _():
            for copy in home_copies(who):
                copy.wait_send()

        @pl.when(c != b)
        def _():
            cross_copy(who).wait_send()
            for copy in away_copies(who):
                copy.wait_send()

        @pl.when(who != me)
        def _():
            for u in range(len(units)):
                dr_copy(u, who).wait_send()

        return carry

    lax.fori_loop(0, n_sp, drain, 0)
    for u in range(len(units)):
        for i in range(1, planes):
            xr_copy(u, i).wait_send()
        for q in range(2):
            for j in range(dests):

                @pl.when(2 * j + c != z)
                def _(u=u, q=q, j=j):
                    z_copy(u, q, j).wait_send()

    @pl.when(c == b)
    def _():
        for u in range(len(units)):
            for q in range(2):
                xo_copy(u, q).wait_send()
                do_copy(u, q).wait_send()

    for copy in rim_copies:
        copy.wait_send()
    for k in range(strips):
        side_copy(k).wait_send()
        copies = ag_copies(k)
        copies[0].wait_send()
        copies[1].wait_send()

        @pl.when(c != b)
        def _(k=k, copies=copies):
            copies[2].wait_send()
            for pc in range(2):
                passed_on(pc, k).wait_send()

    @pl.when(tail)
    def _():
        for copy in halo_copies:
            copy.wait_send()

    for copy in beside_copies:
        copy.wait_send()

    @pl.when(b == 0)
    def _():
        for copy in mate_copies:
            copy.wait_send()

    for j in range(1, pairs):
        for side in range(2):

            @pl.when(jnp.logical_and(b == 1, own_pair < j))
            def _(j=j, side=side):
                for copy in quad_copies(j, side):
                    copy.wait_send()


def fused_shards(n_sp, n_tp, *args):
    (
        res, rv, xf, bf, cf, dt, doff, fade, elf, byp, xk, bk, ck, csv, mm, g1, v, w, s, vk, wk, g2
    ) = args
    f32, bf16 = jnp.float32, jnp.bfloat16
    rows, inner = xf.shape
    heads = dt.shape[1]
    width = mm.shape[1]
    ff = v.shape[1]
    own_rows = rows // n_tp
    row = lambda a: a.reshape(1, -1)
    half = n_sp // 2
    planes = n_sp // FAN
    units = sum(CUTS)
    vmem = pl.BlockSpec(memory_space=pltpu.VMEM)
    hbm = pl.BlockSpec(memory_space=pl.ANY)
    dma = pltpu.SemaphoreType.DMA
    return pl.pallas_call(
        functools.partial(layer_kernel, n_sp, n_tp),
        out_shape=jax.ShapeDtypeStruct(res.shape, bf16),
        in_specs=[hbm] * 2 + [vmem] * 12 + [hbm, vmem] + [hbm] * 3 + [vmem] * 3,
        out_specs=vmem,
        scratch_shapes=[
            pltpu.VMEM((n_sp * v.shape[0], ff), bf16),
            pltpu.VMEM((n_sp * v.shape[0], ff), bf16),
            pltpu.VMEM((n_sp,) + s.shape, bf16),
            pltpu.VMEM((RIM, inner), bf16),
            pltpu.VMEM((RIM, STATE), bf16),
            pltpu.VMEM((RIM, STATE), bf16),
            pltpu.VMEM(vk.shape, bf16),
            pltpu.VMEM(wk.shape, bf16),
            pltpu.VMEM((rows + RIM, 128), f32),
            pltpu.VMEM((rows, inner), bf16),
            pltpu.VMEM((rows, STATE), bf16),
            pltpu.VMEM((rows, STATE), bf16),
            pltpu.VMEM((heads, rows), f32),
            pltpu.VMEM((heads, rows), f32),
            pltpu.VMEM((rows, inner), f32),
            pltpu.VMEM((rows, heads), f32),
            pltpu.VMEM((8, heads), f32),
            pltpu.VMEM((STATE, inner), f32),
            pltpu.VMEM((STATE, inner), bf16),
            pltpu.VMEM((8, heads), f32),
            pltpu.VMEM((STATE, inner), bf16),
            pltpu.VMEM((8, heads), f32),
            pltpu.VMEM((half, STATE, inner), bf16),
            pltpu.VMEM((half, 8, heads), f32),
            pltpu.VMEM((rows, width), bf16),
            pltpu.VMEM((2, own_rows, width), bf16),
            pltpu.VMEM((own_rows, width), bf16),
            pltpu.VMEM((own_rows, width), bf16),
            pltpu.VMEM((own_rows, width), bf16),
            pltpu.VMEM((3, own_rows, width), bf16),
            pltpu.VMEM((2 * own_rows, width), bf16),
            pltpu.VMEM((rows + RIM, width), bf16),
            pltpu.VMEM((rows, ff), bf16),
            pltpu.VMEM(res.shape, bf16),
            pltpu.VMEM(rv.shape, bf16),
            pltpu.VMEM(mm.shape, bf16),
            dma((3,)),
            dma((3,)),
            dma((units, 2, n_sp)),
            dma((units, 2, planes // 2)),
            dma((units, 2)),
            dma((units, 2)),
            dma((units, planes)),
            dma((units, n_sp)),
            dma((3,)),
            dma((3,)),
            dma((2,)),
            dma((2,)),
            dma((2 + planes, 2)),
            dma((half, 2)),
            dma((2,)),
            dma((2,)),
            dma((2,)),
            dma((2,)),
            dma((3, 2)),
            dma((n_tp, 2)),
            dma((2, 2)),
            dma((4,)),
            dma,
            dma((3, n_sp)),
            dma((3, n_sp)),
            dma((n_sp,)),
            dma((n_sp,)),
        ],
        compiler_params=pltpu.CompilerParams(
            collective_id=0, has_side_effects=True, vmem_limit_bytes=60 * 1024 * 1024
        ),
    )(
        res, rv, xf, bf, cf, dt.T, row(doff), row(fade), elf.T, row(byp), xk, bk, ck, row(csv), mm,
        row(g1), v, w, s, vk, wk, row(g2),
    )


def shards_for(n_sp, n_tp):
    def shards(*args):
        rows = args[2].shape[0]
        fits = (
            args[3].shape[1] == STATE
            and args[18].shape[1] % 128 == 0
            and args[16].shape[0] % 64 == 0
            and args[16].shape[1] % 128 == 0
            and n_sp % (2 * FAN) == 0
            and n_sp > 2 * FAN
            and n_tp == 4
            and args[18].shape[0] % 64 == 0
            and rows % (BLOCK * n_tp) == 0
        )
        if fits:
            return fused_shards(n_sp, n_tp, *args)
        return plain_shards(*args)

    return shards


def solution(mesh):
    in_specs = (
        P(("sp", "tp"), None),
        P("sp", "tp"),
        P("sp", "tp"),
        P("sp", "tp"),
        P("sp", "tp"),
        P("sp", "tp"),
        P("tp"),
        P("tp"),
        P("sp", "tp"),
        P("tp"),
        P(None, "tp"),
        P(None, "tp"),
        P(None, "tp"),
        P("tp"),
        P("tp", None),
        P(),
        P("sp", "tp"),
        P("sp", "tp"),
        P("tp", "sp"),
        P(None, "tp"),
        P(None, "tp"),
        P(),
    )
    out_specs = P(("sp", "tp"), None)
    shards = shards_for(mesh.shape["sp"], mesh.shape["tp"])
    return jax.shard_map(shards, mesh=mesh, in_specs=in_specs, out_specs=out_specs, check_vma=False)
```

```python
import functools
import jax
import jax.numpy as jnp
from jax import lax
from jax.experimental import pallas as pl
from jax.experimental.pallas import tpu as pltpu
from jax.sharding import PartitionSpec as P

HEADS = 32
HEAD_DIM = 64
GROUPS = 4
STATE = 128
CONV = 4
FCONV = 3
BLOCK = 128


EPSILON = 1e-05
ALPHA = 2.0**0.25
HIGHEST = lax.Precision.HIGHEST


def shifted(shard, axis, by):
    count = lax.axis_size(axis)
    pairs = [(i, i + by) for i in range(count) if 0 <= i + by < count]
    return lax.ppermute(shard, axis, pairs)


def entering(shard, axis, join, neutral):
    place = lax.axis_index(axis)
    gathered = jax.tree.map(
        lambda a, kind: lax.all_gather(a.astype(kind), axis), shard, (jnp.bfloat16, jnp.bfloat16)
    )
    state = jax.tree.map(lambda a, e: jnp.zeros_like(a) + jnp.asarray(e, a.dtype), shard, neutral)

    def one(lap, state):
        return join(
            state,
            jax.tree.map(
                lambda a, own: lax.dynamic_index_in_dim(a, lap, 0, False).astype(own.dtype),
                gathered,
                shard,
            ),
        )

    return lax.fori_loop(0, place, one, state)


def causal_conv(signal, before, tap_weights):
    tap_count = tap_weights.shape[0]
    row_count = signal.shape[0]
    padded = jnp.concatenate([before, signal], axis=0).astype(jnp.float32)
    running = jnp.zeros(signal.shape, jnp.float32)
    for tap_index in range(tap_count):
        running = (
            running
            + tap_weights[tap_index].astype(jnp.float32) * padded[tap_index : tap_index + row_count]
        )
    return running


def layer_norm(values, scales):
    row_mean = jnp.mean(values, axis=-1, keepdims=True)
    centred = values - row_mean
    spread = jnp.mean(centred * centred, axis=-1, keepdims=True)
    return centred * lax.rsqrt(spread + EPSILON) * scales


def combine_states(earlier_pair, later_pair):
    return (
        earlier_pair[0] * later_pair[1][..., None, None] + later_pair[0],
        earlier_pair[1] * later_pair[1],
    )


def chain_step(state_now, inputs):
    fresh_one, decay_one = inputs
    return (state_now * decay_one[..., None, None] + fresh_one, state_now)


def plain_shards(
    incoming_residual_stream,
    result_valve,
    channel_feed_matrix,
    memory_feed_matrix,
    memory_query_matrix,
    unsoftened_deltas,
    delta_offset,
    channel_fading_speed,
    extra_log_fading,
    bypass_factor,
    channel_feed_kernel,
    memory_feed_kernel,
    memory_query_kernel,
    cluster_scaling_vector,
    mixer_result_matrix,
    initial_scaling_vector,
    valve_matrix,
    widen_matrix,
    shrink_matrix,
    valve_filter_kernel,
    widen_filter_kernel,
    latter_scaling_vector,
):
    row_count = channel_feed_matrix.shape[0]
    inner_here = channel_feed_matrix.shape[1]
    group_count = memory_feed_matrix.shape[1] // STATE
    group_heads = HEADS // GROUPS
    block_count = row_count // BLOCK
    rim_rows = CONV - 1
    rim_x, rim_b, rim_c = shifted(
        (
            channel_feed_matrix[row_count - rim_rows :],
            memory_feed_matrix[row_count - rim_rows :],
            memory_query_matrix[row_count - rim_rows :],
        ),
        "sp",
        1,
    )
    x_act = jax.nn.silu(causal_conv(channel_feed_matrix, rim_x, channel_feed_kernel)).astype(
        jnp.bfloat16
    )
    b_act = jax.nn.silu(causal_conv(memory_feed_matrix, rim_b, memory_feed_kernel)).astype(
        jnp.bfloat16
    )
    c_act = jax.nn.silu(causal_conv(memory_query_matrix, rim_c, memory_query_kernel)).astype(
        jnp.bfloat16
    )
    channel_delta_amount = jax.nn.softplus(unsoftened_deltas + delta_offset[None, :])
    log_fading_amount = extra_log_fading - channel_fading_speed[None, :] * channel_delta_amount
    x_heads = x_act.astype(jnp.float32).reshape(row_count, group_count, group_heads, HEAD_DIM)
    x_scaled = (
        x_heads * channel_delta_amount.reshape(row_count, group_count, group_heads)[..., None]
    )
    b_full = b_act.astype(jnp.float32).reshape(row_count, group_count, STATE)
    c_full = c_act.astype(jnp.float32).reshape(row_count, group_count, STATE)
    decay_full = log_fading_amount.reshape(row_count, group_count, group_heads)
    x_blk = x_scaled.reshape(block_count, BLOCK, group_count, group_heads, HEAD_DIM)
    b_blk = b_full.reshape(block_count, BLOCK, group_count, STATE)
    c_blk = c_full.reshape(block_count, BLOCK, group_count, STATE)
    b_narrow = b_act.reshape(block_count, BLOCK, group_count, STATE)
    c_narrow = c_act.reshape(block_count, BLOCK, group_count, STATE)
    decay_blk = decay_full.reshape(block_count, BLOCK, group_count, group_heads)
    cum_decay = jnp.cumsum(decay_blk, axis=1)
    causal = jnp.tril(jnp.ones((BLOCK, BLOCK), dtype=bool))
    between = cum_decay[:, :, None] - cum_decay[:, None, :]
    lag = jnp.exp(jnp.where(causal[None, :, :, None, None], between, -jnp.inf))
    affinity = jnp.einsum("blgn,bsgn->blsg", c_narrow, b_narrow, preferred_element_type=jnp.float32)
    mixing = affinity[..., None] * lag
    within = jnp.einsum("blsgh,bsghp->blghp", mixing, x_blk, precision=HIGHEST)
    to_end = jnp.exp(cum_decay[:, -1:] - cum_decay)
    fresh = jnp.einsum("blgn,blghp->bghpn", b_blk, x_blk * to_end[..., None], precision=HIGHEST)
    block_decay = jnp.exp(cum_decay[:, -1])
    initial = jnp.zeros((group_count, group_heads, HEAD_DIM, STATE), jnp.float32)
    local_end, earlier = lax.scan(chain_step, initial, (fresh, block_decay))
    carried = (
        jnp.einsum("blgn,bghpn->blghp", c_blk, earlier, precision=HIGHEST)
        * jnp.exp(cum_decay)[..., None]
    )
    from_start = jnp.cumsum(decay_full, axis=0)
    incoming, _ = entering(
        (local_end, jnp.exp(from_start[-1])),
        "sp",
        combine_states,
        (jnp.zeros_like(local_end), jnp.ones_like(from_start[-1])),
    )
    arriving = (
        jnp.einsum("tgn,ghpn->tghp", c_full, incoming, precision=HIGHEST)
        * jnp.exp(from_start)[..., None]
    )
    y_heads = (within + carried).reshape(row_count, group_count, group_heads, HEAD_DIM) + arriving
    y_heads = y_heads + bypass_factor.reshape(group_count, group_heads)[None, :, :, None] * x_heads
    gated = y_heads.reshape(row_count, group_count, group_heads * HEAD_DIM)
    gated = gated * jax.nn.silu(result_valve.astype(jnp.float32)).reshape(
        row_count, group_count, group_heads * HEAD_DIM
    )
    gated = gated * lax.rsqrt(jnp.mean(gated * gated, axis=-1, keepdims=True) + EPSILON)
    y_norm = (gated.reshape(row_count, inner_here) * cluster_scaling_vector[None, :]).astype(
        jnp.bfloat16
    )
    mixer = lax.psum_scatter(
        jnp.dot(y_norm, mixer_result_matrix, preferred_element_type=jnp.float32).astype(
            jnp.bfloat16
        ),
        "tp",
        scatter_dimension=0,
        tiled=True,
    ).astype(jnp.float32)
    normed_own = layer_norm(
        ALPHA * incoming_residual_stream.astype(jnp.float32) + mixer, initial_scaling_vector
    ).astype(jnp.bfloat16)
    normed_all = lax.all_gather(normed_own, "tp", axis=0, tiled=True)
    gate_sum = jnp.dot(
        normed_all,
        lax.all_gather(valve_matrix, "sp", axis=0, tiled=True),
        preferred_element_type=jnp.float32,
    )
    up_sum = jnp.dot(
        normed_all,
        lax.all_gather(widen_matrix, "sp", axis=0, tiled=True),
        preferred_element_type=jnp.float32,
    )
    gate_proj = gate_sum.astype(jnp.bfloat16)
    up_proj = up_sum.astype(jnp.bfloat16)
    ffn_rows = FCONV - 1
    rim_gate, rim_up = shifted(
        (gate_proj[row_count - ffn_rows :], up_proj[row_count - ffn_rows :]), "sp", 1
    )
    gate_conv = causal_conv(gate_proj, rim_gate, valve_filter_kernel)
    up_conv = causal_conv(up_proj, rim_up, widen_filter_kernel)
    hidden = (jax.nn.silu(gate_conv) * up_conv).astype(jnp.bfloat16)
    channel_part = jnp.dot(
        hidden,
        lax.all_gather(shrink_matrix, "sp", axis=1, tiled=True),
        preferred_element_type=jnp.float32,
    )
    channel = lax.psum_scatter(
        channel_part.astype(jnp.bfloat16), "tp", scatter_dimension=0, tiled=True
    ).astype(jnp.float32)
    return layer_norm(
        ALPHA * normed_own.astype(jnp.float32) + channel, latter_scaling_vector
    ).astype(jnp.bfloat16)


MESH = pl.DeviceIdType.MESH
RIM = 16
FAN = 2
CUTS = (2, 2, 4)


def silu(v):
    return v / (1.0 + jnp.exp(-v))


def layer_kernel(
    n_sp,
    n_tp,
    res_hbm,
    rv_hbm,
    xf_ref,
    bf_ref,
    cf_ref,
    dt_ref,
    doff_ref,
    fade_ref,
    elf_ref,
    byp_ref,
    xk_ref,
    bk_ref,
    ck_ref,
    csv_ref,
    mm_hbm,
    g1_ref,
    v_hbm,
    w_hbm,
    s_hbm,
    vk_ref,
    wk_ref,
    g2_ref,
    out_ref,
    v_all,
    w_all,
    s_all,
    rim_x,
    rim_b,
    rim_c,
    vk_other,
    wk_other,
    ext,
    x_act,
    b_act,
    c_act,
    step_ref,
    ld_ref,
    y_ref,
    efs_ref,
    base_ref,
    state_ref,
    st_send,
    dec_send,
    pair_send,
    pair_dec,
    st_recv,
    dec_recv,
    part,
    near_recv,
    side_send,
    side_recv,
    own_norm,
    recv2,
    pre_recv,
    normed,
    gate_act,
    hidden,
    res_ref,
    rv_ref,
    mm_ref,
    late_sem,
    own_sem,
    col_recv,
    xvw_recv,
    xs_recv,
    dv_recv,
    ds_recv,
    z_send,
    xo_send,
    do_send,
    xr_send,
    dr_send,
    rim_send,
    rim_recv,
    tap_send,
    tap_recv,
    st_ssem,
    st_rsem,
    a_send,
    a_recv,
    b_send,
    b_recv,
    ag_send,
    ag_recv,
    agr_send,
    halo_send,
    halo_recv,
    t3_send,
    t3_recv,
    p_send,
    p_recv,
):
    f32, bf16 = jnp.float32, jnp.bfloat16
    rows, inner = xf_ref.shape
    heads = dt_ref.shape[0]
    own_rows = rows // n_tp
    width = mm_hbm.shape[1]
    ff = v_hbm.shape[1]
    depth = v_hbm.shape[0]
    cols = s_hbm.shape[1]
    blocks = rows // BLOCK
    planes = n_sp // FAN
    dests = planes // 2
    half = n_sp // 2
    me = lax.axis_index("sp")
    mt = lax.axis_index("tp")
    z, x = me // FAN, me % FAN
    y, c = mt // 2, mt % 2
    b = z % 2
    mate = z + 1 - 2 * b
    pair0 = z - b

    def dev(pz, px, py, pc):
        return (pz * FAN + px, py * 2 + pc)

    def remote(src, dst, send, recv, device):
        return pltpu.make_async_remote_copy(
            src_ref=src, dst_ref=dst, send_sem=send, recv_sem=recv, device_id=device, device_id_type=MESH
        )

    barrier = pltpu.get_barrier_semaphore()
    total_devices = n_sp * n_tp
    line = me * n_tp + mt
    for d in range(1, total_devices):
        who = (line + d) % total_devices
        pl.semaphore_signal(barrier, inc=1, device_id=(who // n_tp, who % n_tp), device_id_type=MESH)
    pl.semaphore_wait(barrier, total_devices - 1)

    units = [(kind, g) for kind in range(3) for g in range(CUTS[kind])]
    sources = (v_hbm, w_hbm, s_hbm)

    def place(u, q):
        kind, g = units[u]
        size = (ff if kind == 2 else depth) // (2 * CUTS[kind])
        return size, (q * CUTS[kind] + g) * size

    def own_piece(u, q):
        size, at = place(u, q)
        return sources[units[u][0]].at[pl.ds(pl.multiple_of(at, 16), size)]

    def slot(u, q, who):
        size, at = place(u, q)
        kind = units[u][0]
        if kind == 2:
            return s_all.at[who, pl.ds(pl.multiple_of(at, 16), size)]
        whole = v_all if kind == 0 else w_all
        return whole.at[pl.ds(pl.multiple_of(who * depth + at, 16), size)]

    wide = [u for u, (kind, g) in enumerate(units) if kind < 2]
    shrink = [u for u, (kind, g) in enumerate(units) if kind == 2]

    def x_sem(u, pz):
        return xvw_recv.at[u] if u in wide else xs_recv.at[pz]

    def d_sem(u, who):
        return dv_recv.at[units[u][0]] if u in wide else ds_recv.at[who]

    def arrived(sem, count):
        here = v_all.at[pl.ds(0, count)]
        remote(here, here, do_send, sem, dev(z, x, y, 1 - c)).wait_recv()

    def left(sem, count):
        here = v_all.at[pl.ds(0, count)]
        remote(here, here, sem, dv_recv.at[0], dev(z, x, y, 1 - c)).wait_send()

    def z_copy(u, q, j):
        return remote(
            own_piece(u, q), slot(u, q, me), z_send.at[j], col_recv.at[u, z], dev(2 * j + c, x, y, q)
        )

    def xo_copy(u, q):
        return remote(own_piece(u, q), slot(u, q, me), xo_send, x_sem(u, z), dev(z, 1 - x, y, q))

    def do_copy(u, q):
        return remote(own_piece(u, q), slot(u, q, me), do_send, d_sem(u, me), dev(z, x, y, 1 - c))

    def xr_copy(u, i):
        here = slot(u, c, plane_at(i) * FAN + x)
        return remote(here, here, xr_send, x_sem(u, plane_at(i)), dev(z, 1 - x, y, c))

    def dr_copy(u, who, side):
        here = slot(u, c, who)
        return remote(here, here, dr_send.at[side], d_sem(u, who), dev(z, x, y, 1 - c))

    def plane_at(i):
        if i == 0:
            return z
        low = jnp.where(z < planes // 2, z, planes - 1 - z)
        got = jnp.where(i - 1 < low, i - 1, i)
        return jnp.where(z < planes // 2, got, planes - 1 - got)

    def send_z(pieces, only=True):
        for u, q in pieces:
            for j in range(dests):

                @pl.when(jnp.logical_and(2 * j + c != z, only if only is True else only(2 * j + c)))
                def _(u=u, q=q, j=j):
                    z_copy(u, q, j).start()

    def both(us):
        return [(u, q) for u in us for q in range(2)]

    def held(to):
        return jnp.logical_and(jnp.logical_and(b == 0, to > z + 1), z < planes - 2)

    def free(to):
        return jnp.logical_not(held(to))

    def send_xo(which):
        @pl.when(c == b)
        def _():
            for u in which:
                for q in range(2):
                    xo_copy(u, q).start()

    def relay_col(u, picks=None):
        for i in picks or range(1, planes):
            who = plane_at(i) * FAN + x
            here = slot(u, c, who)
            remote(
                here, here, do_send, col_recv.at[u, plane_at(i)], dev(z, x, y, 1 - c)
            ).wait_recv()
            xr_copy(u, i).start()
            dr_copy(u, who, 0).start()

    def relay_x(u):
        arrived(xvw_recv.at[u], planes * place(u, 0)[0])
        for i in range(planes):
            dr_copy(u, plane_at(i) * FAN + 1 - x, 1).start()

    def relay_xs(i):
        arrived(xs_recv.at[plane_at(i)], depth // 2)
        for u in shrink:
            dr_copy(u, plane_at(i) * FAN + 1 - x, 1).start()

    def complete(kind):
        rest = (n_sp - 1) * depth // 2

        @pl.when(c == b)
        def _():
            arrived(dv_recv.at[kind], rest)

        @pl.when(c != b)
        def _():
            arrived(dv_recv.at[kind], rest + depth)

    rim_copies = []
    for i, (src, dst) in enumerate(((xf_ref, rim_x), (bf_ref, rim_b), (cf_ref, rim_c))):
        rim_copies.append(
            remote(
                src.at[pl.ds(rows - RIM, RIM)],
                dst,
                rim_send.at[i],
                rim_recv.at[i],
                ((me + 1) % n_sp, mt),
            )
        )
        rim_copies[-1].start()
    tap_copies = [
        remote(src, dst, tap_send.at[i], tap_recv.at[i], dev(z, x, y, 1 - c))
        for i, (src, dst) in enumerate(((vk_ref, vk_other), (wk_ref, wk_other)))
    ]
    for copy in tap_copies:
        copy.start()
    send_z(both([0]))
    send_xo([0, 1])

    own_copies = []
    for kind in range(3):
        dst = s_all.at[me] if kind == 2 else (v_all, w_all)[kind].at[
            pl.ds(pl.multiple_of(me * depth, 16), depth)
        ]
        own_copies.append(pltpu.make_async_copy(sources[kind], dst, own_sem.at[kind]))

    @pl.when(c == b)
    def _():
        for u in range(len(units)):
            for q in range(2):
                do_copy(u, q).start()
        for copy in own_copies:
            copy.start()

    late = [
        pltpu.make_async_copy(src, dst, late_sem.at[i])
        for i, (src, dst) in enumerate(((rv_hbm, rv_ref), (mm_hbm, mm_ref), (res_hbm, res_ref)))
    ]
    for copy in late:
        copy.start()

    eye = lax.broadcasted_iota(jnp.int32, (heads, heads), 0) == lax.broadcasted_iota(
        jnp.int32, (heads, heads), 1
    )

    def column(a):
        return jnp.sum(jnp.where(eye, a[...], 0.0), axis=1, keepdims=True)

    raw = dt_ref[...] + column(doff_ref)
    step_ref[...] = jnp.maximum(raw, 0.0) + jnp.log1p(jnp.exp(-jnp.abs(raw)))
    ld_ref[...] = elf_ref[...] - column(fade_ref) * step_ref[...]

    for copy in rim_copies:
        copy.wait_recv()
    first = me == 0
    for rim, feed, taps, act in (
        (rim_x, xf_ref, xk_ref, x_act),
        (rim_b, bf_ref, bk_ref, b_act),
        (rim_c, cf_ref, ck_ref, c_act),
    ):
        for lo in range(0, feed.shape[1], 128):
            here = slice(lo, lo + 128)
            edge = rim[:, here].astype(f32)
            ext[0:RIM, :] = jnp.where(first, jnp.zeros_like(edge), edge)
            ext[RIM:, :] = feed[:, here].astype(f32)
            tap = taps[:, here].astype(f32)
            total = jnp.zeros((rows, 128), f32)
            for k in range(CONV):
                start = RIM - (CONV - 1) + k
                total = total + tap[k : k + 1] * ext[start : start + rows, :]
            act[:, here] = silu(total).astype(bf16)

    li = lax.broadcasted_iota(jnp.int32, (BLOCK, BLOCK), 0)
    si = lax.broadcasted_iota(jnp.int32, (BLOCK, BLOCK), 1)
    causal = li >= si
    lower = jnp.where(causal, 1.0, 0.0).astype(f32)
    upper = jnp.where(li <= si, 1.0, 0.0).astype(f32)
    spread = jnp.where(
        lax.broadcasted_iota(jnp.int32, (heads, inner), 1) // HEAD_DIM
        == lax.broadcasted_iota(jnp.int32, (heads, inner), 0),
        1.0,
        0.0,
    ).astype(f32)
    near = lax.broadcasted_iota(jnp.int32, (BLOCK, 2 * HEAD_DIM), 1) < HEAD_DIM

    def widen(a):
        return jnp.dot(a, spread, precision=HIGHEST, preferred_element_type=f32)

    state_ref[...] = jnp.zeros_like(state_ref)
    base_ref[...] = jnp.zeros_like(base_ref)
    skip = widen(byp_ref[...])

    def scan_block(i, carry):
        at = pl.ds(pl.multiple_of(i * BLOCK, BLOCK), BLOCK)
        ld = ld_ref[:, at]
        cum = lax.dot_general(
            lower, ld, (((1,), (1,)), ((), ())), precision=HIGHEST, preferred_element_type=f32
        )
        cum_t = jnp.dot(ld, upper, precision=HIGHEST, preferred_element_type=f32)
        last = cum[BLOCK - 1 : BLOCK, :]
        xx = x_act[at, :].astype(f32)
        bb = b_act[at, :]
        cc = c_act[at, :]
        xs = xx * lax.dot_general(
            step_ref[:, at],
            spread,
            (((0,), (0,)), ((), ())),
            precision=HIGHEST,
            preferred_element_type=f32,
        )
        xs16 = xs.astype(bf16)
        aff = lax.dot_general(
            cc, bb, (((1,), (1,)), ((), ())), preferred_element_type=f32
        )
        yy = (
            jnp.dot(cc, state_ref[...].astype(bf16), preferred_element_type=f32)
            * widen(jnp.exp(cum))
            + skip * xx
        )
        for pair in range(heads // 2):
            at_pair = slice(pair * 2 * HEAD_DIM, (pair + 1) * 2 * HEAD_DIM)
            both = []
            for h in (2 * pair, 2 * pair + 1):
                gap = cum[:, h : h + 1] - cum_t[h : h + 1, :]
                lag = jnp.exp(jnp.where(causal, gap, -1e30))
                both.append(
                    jnp.dot(
                        (aff * lag).astype(bf16), xs16[:, at_pair], preferred_element_type=f32
                    )
                )
            y_ref[at, at_pair] = yy[:, at_pair] + jnp.where(near, both[0], both[1])
        fresh = lax.dot_general(
            bb,
            (xs * widen(jnp.exp(last - cum))).astype(bf16),
            (((0,), (0,)), ((), ())),
            preferred_element_type=f32,
        )
        state_ref[...] = state_ref[...] * widen(jnp.exp(last)) + fresh
        base = base_ref[0:1, :]
        efs_ref[at, :] = jnp.exp(base + cum)
        base_ref[0:1, :] = base + last
        return carry

    lax.fori_loop(0, blocks, scan_block, 0)
    st_send[...] = state_ref[...].astype(bf16)
    dec_send[...] = jnp.broadcast_to(base_ref[0:1, :], dec_send.shape)
    odd = me % 2
    partner = me + 1 - 2 * odd

    pairs = planes // 2
    own_pair = z // 2

    def state_copy(src, src_dec, at, sent, device):
        return [
            remote(a, o.at[at], st_ssem.at[sent, i], st_rsem.at[at, i], device)
            for i, (a, o) in enumerate(((src, st_recv), (src_dec, dec_recv)))
        ]

    beside_copies = state_copy(st_send, dec_send, 0, 0, (partner, mt))
    mate_copies = state_copy(pair_send, pair_dec, 1, 1, dev(mate, x, y, c))

    def quad_copies(j, side):
        to = jnp.minimum(2 * j + side, planes - 1)
        return state_copy(pair_send, pair_dec, 2 + own_pair, 2 + 2 * j + side, dev(to, x, y, c))

    for copy in beside_copies:
        copy.start()
    for copy in beside_copies:
        copy.wait_recv()
    own_dec = widen(jnp.exp(dec_send[0:1, :]))
    beside_dec = widen(jnp.exp(dec_recv[0, 0:1, :]))
    beside = st_recv[0].astype(f32)
    later = odd == 1
    plane_state = jnp.where(
        later, state_ref[...] + beside * own_dec, state_ref[...] * beside_dec + beside
    )

    @pl.when(b == 0)
    def _():
        pair_send[...] = plane_state.astype(bf16)
        pair_dec[...] = dec_send[...] + dec_recv[0]
        for copy in mate_copies:
            copy.start()

    @pl.when(b == 1)
    def _():
        for copy in mate_copies:
            copy.wait_recv()
        plane_dec = dec_send[...] + dec_recv[0]
        pair_send[...] = (
            st_recv[1].astype(f32) * widen(jnp.exp(plane_dec[0:1, :])) + plane_state
        ).astype(bf16)
        pair_dec[...] = plane_dec + dec_recv[1]
        for j in range(1, pairs):
            for side in (1, 0):

                @pl.when(own_pair < j)
                def _(j=j, side=side):
                    for copy in quad_copies(j, side):
                        copy.start()

    state_ref[...] = jnp.zeros_like(state_ref)
    send_z(both([1, 2]), free)
    send_xo(range(2, len(units)))

    def join(at):
        state_ref[...] = state_ref[...] * widen(jnp.exp(dec_recv[at, 0:1, :])) + st_recv[at].astype(f32)

    for j in range(pairs - 1):

        @pl.when(own_pair > j)
        def _(j=j):
            for copy in state_copy(pair_send, pair_dec, 2 + j, 0, dev(mate, x, y, c)):
                copy.wait_recv()
            join(2 + j)

    @pl.when(b == 1)
    def _():
        join(1)

    @pl.when(odd == 1)
    def _():
        join(0)

    for copy in late:
        copy.wait()

    def project_block(i, carry):
        at = pl.ds(pl.multiple_of(i * BLOCK, BLOCK), BLOCK)
        yy = y_ref[at, :] + jnp.dot(
            c_act[at, :], state_ref[...].astype(bf16), preferred_element_type=f32
        ) * widen(efs_ref[at, :])
        gated = yy * silu(rv_ref[at, :].astype(f32))
        gated = gated * lax.rsqrt(jnp.mean(gated * gated, axis=-1, keepdims=True) + EPSILON)
        y_norm = (gated * csv_ref[...]).astype(bf16)
        part[at, :] = jnp.dot(y_norm, mm_ref[...], preferred_element_type=f32).astype(bf16)
        return carry

    def rows_of(t):
        return pl.ds(pl.multiple_of(t * own_rows, own_rows), own_rows)

    def near_copy(py):
        return remote(
            part.at[rows_of(py * 2 + 1 - c)],
            near_recv.at[py],
            a_send.at[py],
            a_recv.at[py],
            dev(z, x, y, 1 - c),
        )

    halfway = blocks // 2
    lax.fori_loop((1 - y) * halfway, (2 - y) * halfway, project_block, 0)
    near_copy(1 - y).start()
    lax.fori_loop(y * halfway, (y + 1) * halfway, project_block, 0)
    near_copy(y).start()

    strips = 2
    strip = own_rows // strips

    def side_copy(k):
        at = pl.ds(k * strip, strip)
        return remote(
            side_send.at[at], side_recv.at[at], b_send.at[k], b_recv.at[k], dev(z, x, 1 - y, c)
        )

    near_copy(1 - y).wait_recv()
    for k in range(strips):
        away = pl.ds(pl.multiple_of(((1 - y) * 2 + c) * own_rows + k * strip, strip), strip)
        side_send[k * strip : (k + 1) * strip, :] = (
            part[away, :].astype(f32) + near_recv[1 - y, k * strip : (k + 1) * strip, :].astype(f32)
        ).astype(bf16)
        side_copy(k).start()
    near_copy(y).wait_recv()
    relay_col(0)

    def ag_copies(k):
        lo = pl.ds(k * strip, strip)
        to = normed.at[pl.ds(pl.multiple_of(RIM + mt * own_rows + k * strip, RIM), strip)]
        return [
            remote(own_norm.at[lo], to, ag_send.at[i, k], ag_recv.at[mt, k], device)
            for i, device in enumerate((dev(mate, x, y, b), dev(z, x, 1 - y, b), dev(z, x, y, b)))
        ]

    for k in range(strips):
        side_copy(k).wait_recv()
        lo = slice(k * strip, (k + 1) * strip)
        mine = pl.ds(pl.multiple_of(mt * own_rows + k * strip, strip), strip)
        mixer = (
            part[mine, :].astype(f32)
            + near_recv[y, lo, :].astype(f32)
            + side_recv[lo, :].astype(f32)
        )
        own_norm[lo, :] = layer_norm(
            ALPHA * res_ref[lo, :].astype(f32) + mixer, g1_ref[...]
        ).astype(bf16)
        copies = ag_copies(k)
        copies[0].start()
        copies[1].start()

        @pl.when(c != b)
        def _(copies=copies):
            copies[2].start()

        @pl.when(c == b)
        def _(k=k, lo=lo):
            normed[pl.ds(pl.multiple_of(RIM + mt * own_rows + k * strip, RIM), strip), :] = own_norm[
                lo, :
            ]

    nxt = me + 1
    nz, nx = nxt // FAN, nxt % FAN
    tail = jnp.logical_and(mt == n_tp - 1, nxt < n_sp)
    halo_copies = [
        remote(
            own_norm.at[pl.ds(own_rows - RIM, RIM)],
            normed.at[pl.ds(0, RIM)],
            halo_send.at[i],
            halo_recv,
            dev(jnp.minimum(nz, planes - 1) // 2 * 2 + i // 2, nx, i % 2, nz % 2),
        )
        for i in range(4)
    ]

    @pl.when(tail)
    def _():
        for copy in halo_copies:
            copy.start()

    send_z(both([1, 2]), held)
    send_z(both([3]))
    outer = jnp.logical_or(z == 0, z == planes - 1)
    def far_outer(to):
        return jnp.logical_and(outer, jnp.abs(to - z) > 1)

    send_z(both(shrink), lambda to: jnp.logical_not(far_outer(to)))

    def gathered(t, k):
        here = normed.at[pl.ds(pl.multiple_of(RIM + t * own_rows + k * strip, RIM), strip)]
        return remote(here, here, ag_send.at[0, 0], ag_recv.at[t, k], dev(z, x, y, 1 - c))

    def passed_on(pc, k):
        here = normed.at[pl.ds(pl.multiple_of(RIM + (y * 2 + pc) * own_rows + k * strip, RIM), strip)]
        return remote(here, here, agr_send.at[pc, k], ag_recv.at[y * 2 + pc, k], dev(z, x, 1 - y, c))

    seg = (pair0 + c) * FAN + x

    relay_col(1)

    @pl.when(c != b)
    def _():
        for k in range(strips):
            for pc in range(2):
                gathered(y * 2 + pc, k).wait_recv()
                passed_on(pc, k).start()

    relay_col(2)
    relay_col(3)
    @pl.when(seg == 0)
    def _():
        normed[0:RIM, :] = jnp.zeros((RIM, width), bf16)

    @pl.when(seg > 0)
    def _():
        halo_copies[0].wait_recv()

    for k in range(strips):

        @pl.when(c == b)
        def _(k=k):
            gathered(y * 2 + 1 - c, k).wait_recv()

        for pc in range(2):
            gathered((1 - y) * 2 + pc, k).wait_recv()

    for u in range(3):
        relay_x(u)

    @pl.when(c == b)
    def _():
        for copy in own_copies:
            copy.wait()

    for copy in tap_copies:
        copy.wait()
    same = c == b

    def conv_cols(at, weights, taps, others):
        proj = jnp.dot(normed[...], weights[:, at], preferred_element_type=f32)
        proj = proj.astype(bf16).astype(f32)
        tap = jnp.where(same, taps[:, at].astype(f32), others[:, at].astype(f32))
        total = jnp.zeros((rows, proj.shape[1]), f32)
        for k in range(FCONV):
            start = RIM - (FCONV - 1) + k
            total = total + tap[k : k + 1] * proj[start : start + rows, :]
        return total

    def gate_cols(at):
        gate_act[:, at] = silu(conv_cols(at, v_all, vk_ref, vk_other))

    def up_cols(at):
        hidden[:, at] = (gate_act[:, at] * conv_cols(at, w_all, wk_ref, wk_other)).astype(bf16)

    chunk = 256
    full = ff // chunk

    def run_cols(fn, lo, hi):
        def one(i, carry):
            fn(pl.ds(pl.multiple_of(i * chunk, chunk), chunk))
            return carry

        lax.fori_loop(lo, hi, one, 0)

    def rest_cols(fn):
        if ff % chunk:
            fn(pl.ds(full * chunk, ff % chunk))

    complete(0)
    run_cols(gate_cols, 0, full)
    rest_cols(gate_cols)
    send_z(both(shrink), lambda to: jnp.logical_and(far_outer(to), to < z))
    relay_x(3)
    complete(1)

    def relay_s(i):
        for u in shrink:
            relay_col(u, [i])

    relay_s(1)
    run_cols(up_cols, 0, full // 2)
    relay_s(2)
    run_cols(up_cols, full // 2, full)
    rest_cols(up_cols)
    send_z(both(shrink), lambda to: jnp.logical_and(far_outer(to), to > z))

    def down(who):
        at = pl.ds(pl.multiple_of(who * cols, cols), cols)
        part[:, at] = jnp.dot(
            hidden[...], s_all[who], preferred_element_type=f32
        ).astype(bf16)

    def at_of(who):
        return pl.ds(pl.multiple_of(who * cols, cols), cols)

    def side_half(py):
        return pl.ds(pl.multiple_of(py * 2 * own_rows, own_rows), 2 * own_rows)

    def home_copies(who):
        at = at_of(who)
        return [
            remote(
                part.at[rows_of(py * 2 + pc), at],
                recv2.at[y, :, at],
                t3_send,
                t3_recv.at[y],
                dev(z, x, py, pc),
            )
            for py, pc in ((1 - y, 0), (1 - y, 1), (y, 1 - c))
        ]

    def cross_copy(who):
        at = at_of(who)
        return remote(
            part.at[side_half(1 - y), at], pre_recv.at[:, at], p_send, p_recv.at[who], dev(z, x, 1 - y, c)
        )

    def away_copies(who):
        at = at_of(who)
        return [
            remote(
                part.at[rows_of(y * 2 + pc), at],
                recv2.at[2, :, at],
                t3_send,
                t3_recv.at[2],
                dev(mate, x, y, pc),
            )
            for pc in range(2)
        ]

    done = []
    lag = 2

    def finish(who):
        at = at_of(who)

        @pl.when(c != b)
        def _():
            cross_copy(who).wait_recv()
            here = side_half(y)
            part[here, at] = (part[here, at].astype(f32) + pre_recv[:, at].astype(f32)).astype(bf16)
            for copy in away_copies(who):
                copy.start()

    def down_step(who):
        down(who)
        at = at_of(who)

        @pl.when(c != b)
        def _():
            cross_copy(who).start()

        @pl.when(c == b)
        def _():
            for copy in home_copies(who):
                copy.start()
            recv2[y, :, at] = part[rows_of(mt), at]

        done.append(who)
        if len(done) > lag:
            finish(done[-1 - lag])

    near_copy(0).wait_send()
    near_copy(1).wait_send()

    @pl.when(c != b)
    def _():
        arrived(ds_recv.at[me], depth)

    down_step(me)

    def x_step(i):
        who = plane_at(i) * FAN + 1 - x
        relay_xs(i)
        arrived(ds_recv.at[who], depth // 2)
        down_step(who)

    def col_step(i):
        who = plane_at(i) * FAN + x
        arrived(ds_recv.at[who], depth // 2)
        down_step(who)

    x_step(0)
    col_step(1)
    last = planes - 1
    relay_col(4, [last])
    relay_col(5, [last])
    x_step(1)
    relay_col(6, [last])
    for i in range(2, last):
        col_step(i)
        if i == 2:
            relay_col(7, [last])
        x_step(i)
    col_step(last)
    x_step(last)
    for who in done[-lag:]:
        finish(who)

    for t in range(3):

        @pl.when(jnp.logical_or(c != b, y != t))
        def _(t=t):
            remote(recv2.at[t], recv2.at[t], t3_send, t3_recv.at[t], dev(z, x, y, 1 - c)).wait_recv()

    channel = recv2[0].astype(f32)
    for t in range(1, 3):
        channel = channel + recv2[t].astype(f32)
    out_ref[...] = layer_norm(
        ALPHA * own_norm[...].astype(f32) + channel, g2_ref[...]
    ).astype(bf16)

    def part_left(sem, count):
        here = part.at[pl.ds(0, count)]
        remote(here, here, sem, t3_recv.at[0], dev(z, x, y, 1 - c)).wait_send()

    @pl.when(c == b)
    def _():
        part_left(t3_send, 3 * own_rows)
        left(xo_send, 3 * depth)
        left(do_send, 3 * depth)

    @pl.when(c != b)
    def _():
        part_left(t3_send, 2 * own_rows)
        part_left(p_send, 2 * own_rows)

    half_blocks = 3 * depth // 2
    left(xr_send, (planes - 1) * half_blocks)
    left(dr_send.at[0], (planes - 1) * half_blocks)
    left(dr_send.at[1], planes * half_blocks)
    for j in range(dests):

        @pl.when(2 * j + c != z)
        def _(j=j):
            left(z_send.at[j], 3 * depth)

    for copy in rim_copies:
        copy.wait_send()
    for k in range(strips):
        side_copy(k).wait_send()
        copies = ag_copies(k)
        copies[0].wait_send()
        copies[1].wait_send()

        @pl.when(c != b)
        def _(k=k, copies=copies):
            copies[2].wait_send()
            for pc in range(2):
                passed_on(pc, k).wait_send()

    @pl.when(tail)
    def _():
        for copy in halo_copies:
            copy.wait_send()

    for copy in beside_copies:
        copy.wait_send()

    @pl.when(b == 0)
    def _():
        for copy in mate_copies:
            copy.wait_send()

    for j in range(1, pairs):
        for side in range(2):

            @pl.when(jnp.logical_and(b == 1, own_pair < j))
            def _(j=j, side=side):
                for copy in quad_copies(j, side):
                    copy.wait_send()


def fused_shards(n_sp, n_tp, *args):
    (
        res, rv, xf, bf, cf, dt, doff, fade, elf, byp, xk, bk, ck, csv, mm, g1, v, w, s, vk, wk, g2
    ) = args
    f32, bf16 = jnp.float32, jnp.bfloat16
    rows, inner = xf.shape
    heads = dt.shape[1]
    width = mm.shape[1]
    ff = v.shape[1]
    own_rows = rows // n_tp
    row = lambda a: a.reshape(1, -1)
    half = n_sp // 2
    planes = n_sp // FAN
    units = sum(CUTS)
    vmem = pl.BlockSpec(memory_space=pltpu.VMEM)
    hbm = pl.BlockSpec(memory_space=pl.ANY)
    dma = pltpu.SemaphoreType.DMA
    return pl.pallas_call(
        functools.partial(layer_kernel, n_sp, n_tp),
        out_shape=jax.ShapeDtypeStruct(res.shape, bf16),
        in_specs=[hbm] * 2 + [vmem] * 12 + [hbm, vmem] + [hbm] * 3 + [vmem] * 3,
        out_specs=vmem,
        scratch_shapes=[
            pltpu.VMEM((n_sp * v.shape[0], ff), bf16),
            pltpu.VMEM((n_sp * v.shape[0], ff), bf16),
            pltpu.VMEM((n_sp,) + s.shape, bf16),
            pltpu.VMEM((RIM, inner), bf16),
            pltpu.VMEM((RIM, STATE), bf16),
            pltpu.VMEM((RIM, STATE), bf16),
            pltpu.VMEM(vk.shape, bf16),
            pltpu.VMEM(wk.shape, bf16),
            pltpu.VMEM((rows + RIM, 128), f32),
            pltpu.VMEM((rows, inner), bf16),
            pltpu.VMEM((rows, STATE), bf16),
            pltpu.VMEM((rows, STATE), bf16),
            pltpu.VMEM((heads, rows), f32),
            pltpu.VMEM((heads, rows), f32),
            pltpu.VMEM((rows, inner), f32),
            pltpu.VMEM((rows, heads), f32),
            pltpu.VMEM((8, heads), f32),
            pltpu.VMEM((STATE, inner), f32),
            pltpu.VMEM((STATE, inner), bf16),
            pltpu.VMEM((8, heads), f32),
            pltpu.VMEM((STATE, inner), bf16),
            pltpu.VMEM((8, heads), f32),
            pltpu.VMEM((half, STATE, inner), bf16),
            pltpu.VMEM((half, 8, heads), f32),
            pltpu.VMEM((rows, width), bf16),
            pltpu.VMEM((2, own_rows, width), bf16),
            pltpu.VMEM((own_rows, width), bf16),
            pltpu.VMEM((own_rows, width), bf16),
            pltpu.VMEM((own_rows, width), bf16),
            pltpu.VMEM((3, own_rows, width), bf16),
            pltpu.VMEM((2 * own_rows, width), bf16),
            pltpu.VMEM((rows + RIM, width), bf16),
            pltpu.VMEM((rows, ff), f32),
            pltpu.VMEM((rows, ff), bf16),
            pltpu.VMEM(res.shape, bf16),
            pltpu.VMEM(rv.shape, bf16),
            pltpu.VMEM(mm.shape, bf16),
            dma((3,)),
            dma((3,)),
            dma((units, planes)),
            dma((CUTS[0] + CUTS[1],)),
            dma((planes,)),
            dma((2,)),
            dma((n_sp,)),
            dma((planes // 2,)),
            dma,
            dma,
            dma,
            dma((2,)),
            dma((3,)),
            dma((3,)),
            dma((2,)),
            dma((2,)),
            dma((2 + planes, 2)),
            dma((half, 2)),
            dma((2,)),
            dma((2,)),
            dma((2,)),
            dma((2,)),
            dma((3, 2)),
            dma((n_tp, 2)),
            dma((2, 2)),
            dma((4,)),
            dma,
            dma,
            dma((3,)),
            dma,
            dma((n_sp,)),
        ],
        compiler_params=pltpu.CompilerParams(
            collective_id=0, has_side_effects=True, vmem_limit_bytes=60 * 1024 * 1024
        ),
    )(
        res, rv, xf, bf, cf, dt.T, row(doff), row(fade), elf.T, row(byp), xk, bk, ck, row(csv), mm,
        row(g1), v, w, s, vk, wk, row(g2),
    )


def shards_for(n_sp, n_tp):
    def shards(*args):
        rows = args[2].shape[0]
        fits = (
            args[3].shape[1] == STATE
            and args[18].shape[1] % 128 == 0
            and args[16].shape[0] % 64 == 0
            and args[16].shape[1] % 128 == 0
            and n_sp % (2 * FAN) == 0
            and n_sp > 2 * FAN
            and n_tp == 4
            and args[18].shape[0] % 128 == 0
            and args[18].shape[::-1] == args[16].shape
            and rows % (BLOCK * n_tp) == 0
        )
        if fits:
            return fused_shards(n_sp, n_tp, *args)
        return plain_shards(*args)

    return shards


def solution(mesh):
    in_specs = (
        P(("sp", "tp"), None),
        P("sp", "tp"),
        P("sp", "tp"),
        P("sp", "tp"),
        P("sp", "tp"),
        P("sp", "tp"),
        P("tp"),
        P("tp"),
        P("sp", "tp"),
        P("tp"),
        P(None, "tp"),
        P(None, "tp"),
        P(None, "tp"),
        P("tp"),
        P("tp", None),
        P(),
        P("sp", "tp"),
        P("sp", "tp"),
        P("tp", "sp"),
        P(None, "tp"),
        P(None, "tp"),
        P(),
    )
    out_specs = P(("sp", "tp"), None)
    shards = shards_for(mesh.shape["sp"], mesh.shape["tp"])
    return jax.shard_map(shards, mesh=mesh, in_specs=in_specs, out_specs=out_specs, check_vma=False)
```

```python
import functools
import jax
import jax.numpy as jnp
from jax import lax
from jax.experimental import pallas as pl
from jax.experimental.pallas import tpu as pltpu
from jax.sharding import PartitionSpec as P

HEADS = 32
HEAD_DIM = 64
GROUPS = 4
STATE = 128
CONV = 4
FCONV = 3
BLOCK = 128


EPSILON = 1e-05
ALPHA = 2.0**0.25
HIGHEST = lax.Precision.HIGHEST


def shifted(shard, axis, by):
    count = lax.axis_size(axis)
    pairs = [(i, i + by) for i in range(count) if 0 <= i + by < count]
    return lax.ppermute(shard, axis, pairs)


def entering(shard, axis, join, neutral):
    place = lax.axis_index(axis)
    gathered = jax.tree.map(
        lambda a, kind: lax.all_gather(a.astype(kind), axis), shard, (jnp.bfloat16, jnp.bfloat16)
    )
    state = jax.tree.map(lambda a, e: jnp.zeros_like(a) + jnp.asarray(e, a.dtype), shard, neutral)

    def one(lap, state):
        return join(
            state,
            jax.tree.map(
                lambda a, own: lax.dynamic_index_in_dim(a, lap, 0, False).astype(own.dtype),
                gathered,
                shard,
            ),
        )

    return lax.fori_loop(0, place, one, state)


def causal_conv(signal, before, tap_weights):
    tap_count = tap_weights.shape[0]
    row_count = signal.shape[0]
    padded = jnp.concatenate([before, signal], axis=0).astype(jnp.float32)
    running = jnp.zeros(signal.shape, jnp.float32)
    for tap_index in range(tap_count):
        running = (
            running
            + tap_weights[tap_index].astype(jnp.float32) * padded[tap_index : tap_index + row_count]
        )
    return running


def layer_norm(values, scales):
    row_mean = jnp.mean(values, axis=-1, keepdims=True)
    centred = values - row_mean
    spread = jnp.mean(centred * centred, axis=-1, keepdims=True)
    return centred * lax.rsqrt(spread + EPSILON) * scales


def combine_states(earlier_pair, later_pair):
    return (
        earlier_pair[0] * later_pair[1][..., None, None] + later_pair[0],
        earlier_pair[1] * later_pair[1],
    )


def chain_step(state_now, inputs):
    fresh_one, decay_one = inputs
    return (state_now * decay_one[..., None, None] + fresh_one, state_now)


def plain_shards(
    incoming_residual_stream,
    result_valve,
    channel_feed_matrix,
    memory_feed_matrix,
    memory_query_matrix,
    unsoftened_deltas,
    delta_offset,
    channel_fading_speed,
    extra_log_fading,
    bypass_factor,
    channel_feed_kernel,
    memory_feed_kernel,
    memory_query_kernel,
    cluster_scaling_vector,
    mixer_result_matrix,
    initial_scaling_vector,
    valve_matrix,
    widen_matrix,
    shrink_matrix,
    valve_filter_kernel,
    widen_filter_kernel,
    latter_scaling_vector,
):
    row_count = channel_feed_matrix.shape[0]
    inner_here = channel_feed_matrix.shape[1]
    group_count = memory_feed_matrix.shape[1] // STATE
    group_heads = HEADS // GROUPS
    block_count = row_count // BLOCK
    rim_rows = CONV - 1
    rim_x, rim_b, rim_c = shifted(
        (
            channel_feed_matrix[row_count - rim_rows :],
            memory_feed_matrix[row_count - rim_rows :],
            memory_query_matrix[row_count - rim_rows :],
        ),
        "sp",
        1,
    )
    x_act = jax.nn.silu(causal_conv(channel_feed_matrix, rim_x, channel_feed_kernel)).astype(
        jnp.bfloat16
    )
    b_act = jax.nn.silu(causal_conv(memory_feed_matrix, rim_b, memory_feed_kernel)).astype(
        jnp.bfloat16
    )
    c_act = jax.nn.silu(causal_conv(memory_query_matrix, rim_c, memory_query_kernel)).astype(
        jnp.bfloat16
    )
    channel_delta_amount = jax.nn.softplus(unsoftened_deltas + delta_offset[None, :])
    log_fading_amount = extra_log_fading - channel_fading_speed[None, :] * channel_delta_amount
    x_heads = x_act.astype(jnp.float32).reshape(row_count, group_count, group_heads, HEAD_DIM)
    x_scaled = (
        x_heads * channel_delta_amount.reshape(row_count, group_count, group_heads)[..., None]
    )
    b_full = b_act.astype(jnp.float32).reshape(row_count, group_count, STATE)
    c_full = c_act.astype(jnp.float32).reshape(row_count, group_count, STATE)
    decay_full = log_fading_amount.reshape(row_count, group_count, group_heads)
    x_blk = x_scaled.reshape(block_count, BLOCK, group_count, group_heads, HEAD_DIM)
    b_blk = b_full.reshape(block_count, BLOCK, group_count, STATE)
    c_blk = c_full.reshape(block_count, BLOCK, group_count, STATE)
    b_narrow = b_act.reshape(block_count, BLOCK, group_count, STATE)
    c_narrow = c_act.reshape(block_count, BLOCK, group_count, STATE)
    decay_blk = decay_full.reshape(block_count, BLOCK, group_count, group_heads)
    cum_decay = jnp.cumsum(decay_blk, axis=1)
    causal = jnp.tril(jnp.ones((BLOCK, BLOCK), dtype=bool))
    between = cum_decay[:, :, None] - cum_decay[:, None, :]
    lag = jnp.exp(jnp.where(causal[None, :, :, None, None], between, -jnp.inf))
    affinity = jnp.einsum("blgn,bsgn->blsg", c_narrow, b_narrow, preferred_element_type=jnp.float32)
    mixing = affinity[..., None] * lag
    within = jnp.einsum("blsgh,bsghp->blghp", mixing, x_blk, precision=HIGHEST)
    to_end = jnp.exp(cum_decay[:, -1:] - cum_decay)
    fresh = jnp.einsum("blgn,blghp->bghpn", b_blk, x_blk * to_end[..., None], precision=HIGHEST)
    block_decay = jnp.exp(cum_decay[:, -1])
    initial = jnp.zeros((group_count, group_heads, HEAD_DIM, STATE), jnp.float32)
    local_end, earlier = lax.scan(chain_step, initial, (fresh, block_decay))
    carried = (
        jnp.einsum("blgn,bghpn->blghp", c_blk, earlier, precision=HIGHEST)
        * jnp.exp(cum_decay)[..., None]
    )
    from_start = jnp.cumsum(decay_full, axis=0)
    incoming, _ = entering(
        (local_end, jnp.exp(from_start[-1])),
        "sp",
        combine_states,
        (jnp.zeros_like(local_end), jnp.ones_like(from_start[-1])),
    )
    arriving = (
        jnp.einsum("tgn,ghpn->tghp", c_full, incoming, precision=HIGHEST)
        * jnp.exp(from_start)[..., None]
    )
    y_heads = (within + carried).reshape(row_count, group_count, group_heads, HEAD_DIM) + arriving
    y_heads = y_heads + bypass_factor.reshape(group_count, group_heads)[None, :, :, None] * x_heads
    gated = y_heads.reshape(row_count, group_count, group_heads * HEAD_DIM)
    gated = gated * jax.nn.silu(result_valve.astype(jnp.float32)).reshape(
        row_count, group_count, group_heads * HEAD_DIM
    )
    gated = gated * lax.rsqrt(jnp.mean(gated * gated, axis=-1, keepdims=True) + EPSILON)
    y_norm = (gated.reshape(row_count, inner_here) * cluster_scaling_vector[None, :]).astype(
        jnp.bfloat16
    )
    mixer = lax.psum_scatter(
        jnp.dot(y_norm, mixer_result_matrix, preferred_element_type=jnp.float32).astype(
            jnp.bfloat16
        ),
        "tp",
        scatter_dimension=0,
        tiled=True,
    ).astype(jnp.float32)
    normed_own = layer_norm(
        ALPHA * incoming_residual_stream.astype(jnp.float32) + mixer, initial_scaling_vector
    ).astype(jnp.bfloat16)
    normed_all = lax.all_gather(normed_own, "tp", axis=0, tiled=True)
    gate_sum = jnp.dot(
        normed_all,
        lax.all_gather(valve_matrix, "sp", axis=0, tiled=True),
        preferred_element_type=jnp.float32,
    )
    up_sum = jnp.dot(
        normed_all,
        lax.all_gather(widen_matrix, "sp", axis=0, tiled=True),
        preferred_element_type=jnp.float32,
    )
    gate_proj = gate_sum.astype(jnp.bfloat16)
    up_proj = up_sum.astype(jnp.bfloat16)
    ffn_rows = FCONV - 1
    rim_gate, rim_up = shifted(
        (gate_proj[row_count - ffn_rows :], up_proj[row_count - ffn_rows :]), "sp", 1
    )
    gate_conv = causal_conv(gate_proj, rim_gate, valve_filter_kernel)
    up_conv = causal_conv(up_proj, rim_up, widen_filter_kernel)
    hidden = (jax.nn.silu(gate_conv) * up_conv).astype(jnp.bfloat16)
    channel_part = jnp.dot(
        hidden,
        lax.all_gather(shrink_matrix, "sp", axis=1, tiled=True),
        preferred_element_type=jnp.float32,
    )
    channel = lax.psum_scatter(
        channel_part.astype(jnp.bfloat16), "tp", scatter_dimension=0, tiled=True
    ).astype(jnp.float32)
    return layer_norm(
        ALPHA * normed_own.astype(jnp.float32) + channel, latter_scaling_vector
    ).astype(jnp.bfloat16)


MESH = pl.DeviceIdType.MESH
RIM = 16
FAN = 2
CUTS = (2, 2, 4)


def silu(v):
    return v / (1.0 + jnp.exp(-v))


def layer_kernel(
    n_sp,
    n_tp,
    res_hbm,
    rv_hbm,
    xf_ref,
    bf_ref,
    cf_ref,
    dt_ref,
    doff_ref,
    fade_ref,
    elf_ref,
    byp_ref,
    xk_ref,
    bk_ref,
    ck_ref,
    csv_ref,
    mm_hbm,
    g1_ref,
    v_hbm,
    w_hbm,
    s_hbm,
    vk_ref,
    wk_ref,
    g2_ref,
    out_ref,
    v_all,
    w_all,
    s_all,
    rim_x,
    rim_b,
    rim_c,
    vk_other,
    wk_other,
    ext,
    x_act,
    b_act,
    c_act,
    step_ref,
    ld_ref,
    y_ref,
    efs_ref,
    base_ref,
    state_ref,
    st_send,
    dec_send,
    pair_send,
    pair_dec,
    st_recv,
    dec_recv,
    part,
    near_recv,
    side_send,
    side_recv,
    own_norm,
    recv2,
    pre_recv,
    normed,
    gate_act,
    hidden,
    res_ref,
    rv_ref,
    mm_ref,
    late_sem,
    own_sem,
    col_recv,
    xvw_recv,
    xs_recv,
    dv_recv,
    ds_recv,
    z_send,
    xo_send,
    do_send,
    xr_send,
    dr_send,
    rim_send,
    rim_recv,
    tap_send,
    tap_recv,
    st_ssem,
    st_rsem,
    a_send,
    a_recv,
    b_send,
    b_recv,
    ag_send,
    ag_recv,
    agr_send,
    halo_send,
    halo_recv,
    t3_send,
    t3_recv,
    p_send,
    p_recv,
):
    f32, bf16 = jnp.float32, jnp.bfloat16
    rows, inner = xf_ref.shape
    heads = dt_ref.shape[0]
    own_rows = rows // n_tp
    width = mm_hbm.shape[1]
    ff = v_hbm.shape[1]
    depth = v_hbm.shape[0]
    cols = s_hbm.shape[1]
    blocks = rows // BLOCK
    planes = n_sp // FAN
    dests = planes // 2
    half = n_sp // 2
    me = lax.axis_index("sp")
    mt = lax.axis_index("tp")
    z, x = me // FAN, me % FAN
    y, c = mt // 2, mt % 2
    b = z % 2
    mate = z + 1 - 2 * b
    pair0 = z - b

    def dev(pz, px, py, pc):
        return (pz * FAN + px, py * 2 + pc)

    def remote(src, dst, send, recv, device):
        return pltpu.make_async_remote_copy(
            src_ref=src, dst_ref=dst, send_sem=send, recv_sem=recv, device_id=device, device_id_type=MESH
        )

    barrier = pltpu.get_barrier_semaphore()
    total_devices = n_sp * n_tp
    line = me * n_tp + mt
    for d in range(1, total_devices):
        who = (line + d) % total_devices
        pl.semaphore_signal(barrier, inc=1, device_id=(who // n_tp, who % n_tp), device_id_type=MESH)
    pl.semaphore_wait(barrier, total_devices - 1)

    units = [(kind, g) for kind in range(3) for g in range(CUTS[kind])]
    sources = (v_hbm, w_hbm, s_hbm)

    def place(u, q):
        kind, g = units[u]
        size = (ff if kind == 2 else depth) // (2 * CUTS[kind])
        return size, (q * CUTS[kind] + g) * size

    def own_piece(u, q):
        size, at = place(u, q)
        return sources[units[u][0]].at[pl.ds(pl.multiple_of(at, 16), size)]

    def slot(u, q, who):
        size, at = place(u, q)
        kind = units[u][0]
        if kind == 2:
            return s_all.at[who, pl.ds(pl.multiple_of(at, 16), size)]
        whole = v_all if kind == 0 else w_all
        return whole.at[pl.ds(pl.multiple_of(who * depth + at, 16), size)]

    wide = [u for u, (kind, g) in enumerate(units) if kind < 2]
    shrink = [u for u, (kind, g) in enumerate(units) if kind == 2]

    def x_sem(u, pz):
        return xvw_recv.at[u] if u in wide else xs_recv.at[pz]

    def d_sem(u, who):
        return dv_recv.at[units[u][0]] if u in wide else ds_recv.at[who]

    def arrived(sem, count):
        here = v_all.at[pl.ds(0, count)]
        remote(here, here, do_send, sem, dev(z, x, y, 1 - c)).wait_recv()

    def left(sem, count):
        here = v_all.at[pl.ds(0, count)]
        remote(here, here, sem, dv_recv.at[0], dev(z, x, y, 1 - c)).wait_send()

    def z_copy(u, q, j):
        return remote(
            own_piece(u, q), slot(u, q, me), z_send.at[j], col_recv.at[u, z], dev(2 * j + c, x, y, q)
        )

    def xo_copy(u, q):
        return remote(own_piece(u, q), slot(u, q, me), xo_send, x_sem(u, z), dev(z, 1 - x, y, q))

    def do_copy(u, q):
        return remote(own_piece(u, q), slot(u, q, me), do_send, d_sem(u, me), dev(z, x, y, 1 - c))

    def xr_copy(u, i):
        here = slot(u, c, plane_at(i) * FAN + x)
        return remote(here, here, xr_send, x_sem(u, plane_at(i)), dev(z, 1 - x, y, c))

    def dr_copy(u, who, side):
        here = slot(u, c, who)
        return remote(here, here, dr_send.at[side], d_sem(u, who), dev(z, x, y, 1 - c))

    def plane_at(i):
        if i == 0:
            return z
        low = jnp.where(z < planes // 2, z, planes - 1 - z)
        got = jnp.where(i - 1 < low, i - 1, i)
        return jnp.where(z < planes // 2, got, planes - 1 - got)

    def send_z(pieces, only=True):
        for u, q in pieces:
            for j in range(dests):

                @pl.when(jnp.logical_and(2 * j + c != z, only if only is True else only(2 * j + c)))
                def _(u=u, q=q, j=j):
                    z_copy(u, q, j).start()

    def both(us):
        return [(u, q) for u in us for q in range(2)]

    def held(to):
        return jnp.logical_and(jnp.logical_and(b == 0, to > z + 1), z < planes - 2)

    def free(to):
        return jnp.logical_not(held(to))

    def send_xo(which):
        @pl.when(c == b)
        def _():
            for u in which:
                for q in range(2):
                    xo_copy(u, q).start()

    def relay_col(u, picks=None):
        for i in picks or range(1, planes):
            who = plane_at(i) * FAN + x
            here = slot(u, c, who)
            remote(
                here, here, do_send, col_recv.at[u, plane_at(i)], dev(z, x, y, 1 - c)
            ).wait_recv()
            xr_copy(u, i).start()
            dr_copy(u, who, 0).start()

    def relay_x(u):
        arrived(xvw_recv.at[u], planes * place(u, 0)[0])
        for i in range(planes):
            dr_copy(u, plane_at(i) * FAN + 1 - x, 1).start()

    def relay_xs(i):
        arrived(xs_recv.at[plane_at(i)], depth // 2)
        for u in shrink:
            dr_copy(u, plane_at(i) * FAN + 1 - x, 1).start()

    def complete(kind):
        rest = (n_sp - 1) * depth // 2

        @pl.when(c == b)
        def _():
            arrived(dv_recv.at[kind], rest)

        @pl.when(c != b)
        def _():
            arrived(dv_recv.at[kind], rest + depth)

    rim_copies = []
    for i, (src, dst) in enumerate(((xf_ref, rim_x), (bf_ref, rim_b), (cf_ref, rim_c))):
        rim_copies.append(
            remote(
                src.at[pl.ds(rows - RIM, RIM)],
                dst,
                rim_send.at[i],
                rim_recv.at[i],
                ((me + 1) % n_sp, mt),
            )
        )
        rim_copies[-1].start()
    tap_copies = [
        remote(src, dst, tap_send.at[i], tap_recv.at[i], dev(z, x, y, 1 - c))
        for i, (src, dst) in enumerate(((vk_ref, vk_other), (wk_ref, wk_other)))
    ]
    for copy in tap_copies:
        copy.start()
    send_z(both([0]))
    send_xo([0, 1])

    own_copies = []
    for kind in range(3):
        dst = s_all.at[me] if kind == 2 else (v_all, w_all)[kind].at[
            pl.ds(pl.multiple_of(me * depth, 16), depth)
        ]
        own_copies.append(pltpu.make_async_copy(sources[kind], dst, own_sem.at[kind]))

    @pl.when(c == b)
    def _():
        for u in range(len(units)):
            for q in range(2):
                do_copy(u, q).start()
        for copy in own_copies:
            copy.start()

    late = [
        pltpu.make_async_copy(src, dst, late_sem.at[i])
        for i, (src, dst) in enumerate(((rv_hbm, rv_ref), (mm_hbm, mm_ref), (res_hbm, res_ref)))
    ]
    for copy in late:
        copy.start()

    eye = lax.broadcasted_iota(jnp.int32, (heads, heads), 0) == lax.broadcasted_iota(
        jnp.int32, (heads, heads), 1
    )

    def column(a):
        return jnp.sum(jnp.where(eye, a[...], 0.0), axis=1, keepdims=True)

    raw = dt_ref[...] + column(doff_ref)
    step_ref[...] = jnp.maximum(raw, 0.0) + jnp.log1p(jnp.exp(-jnp.abs(raw)))
    ld_ref[...] = elf_ref[...] - column(fade_ref) * step_ref[...]

    for copy in rim_copies:
        copy.wait_recv()
    first = me == 0
    for rim, feed, taps, act in (
        (rim_x, xf_ref, xk_ref, x_act),
        (rim_b, bf_ref, bk_ref, b_act),
        (rim_c, cf_ref, ck_ref, c_act),
    ):
        for lo in range(0, feed.shape[1], 128):
            here = slice(lo, lo + 128)
            edge = rim[:, here].astype(f32)
            ext[0:RIM, :] = jnp.where(first, jnp.zeros_like(edge), edge)
            ext[RIM:, :] = feed[:, here].astype(f32)
            tap = taps[:, here].astype(f32)
            total = jnp.zeros((rows, 128), f32)
            for k in range(CONV):
                start = RIM - (CONV - 1) + k
                total = total + tap[k : k + 1] * ext[start : start + rows, :]
            act[:, here] = silu(total).astype(bf16)

    li = lax.broadcasted_iota(jnp.int32, (BLOCK, BLOCK), 0)
    si = lax.broadcasted_iota(jnp.int32, (BLOCK, BLOCK), 1)
    causal = li >= si
    lower = jnp.where(causal, 1.0, 0.0).astype(f32)
    upper = jnp.where(li <= si, 1.0, 0.0).astype(f32)
    spread = jnp.where(
        lax.broadcasted_iota(jnp.int32, (heads, inner), 1) // HEAD_DIM
        == lax.broadcasted_iota(jnp.int32, (heads, inner), 0),
        1.0,
        0.0,
    ).astype(f32)
    near = lax.broadcasted_iota(jnp.int32, (BLOCK, 2 * HEAD_DIM), 1) < HEAD_DIM

    def widen(a):
        return jnp.dot(a, spread, precision=HIGHEST, preferred_element_type=f32)

    state_ref[...] = jnp.zeros_like(state_ref)
    base_ref[...] = jnp.zeros_like(base_ref)
    skip = widen(byp_ref[...])

    def scan_block(i, carry):
        at = pl.ds(pl.multiple_of(i * BLOCK, BLOCK), BLOCK)
        ld = ld_ref[:, at]
        cum = lax.dot_general(
            lower, ld, (((1,), (1,)), ((), ())), precision=HIGHEST, preferred_element_type=f32
        )
        cum_t = jnp.dot(ld, upper, precision=HIGHEST, preferred_element_type=f32)
        last = cum[BLOCK - 1 : BLOCK, :]
        xx = x_act[at, :].astype(f32)
        bb = b_act[at, :]
        cc = c_act[at, :]
        xs = xx * lax.dot_general(
            step_ref[:, at],
            spread,
            (((0,), (0,)), ((), ())),
            precision=HIGHEST,
            preferred_element_type=f32,
        )
        xs16 = xs.astype(bf16)
        aff = lax.dot_general(
            cc, bb, (((1,), (1,)), ((), ())), preferred_element_type=f32
        )
        yy = (
            jnp.dot(cc, state_ref[...].astype(bf16), preferred_element_type=f32)
            * widen(jnp.exp(cum))
            + skip * xx
        )
        for pair in range(heads // 2):
            at_pair = slice(pair * 2 * HEAD_DIM, (pair + 1) * 2 * HEAD_DIM)
            both = []
            for h in (2 * pair, 2 * pair + 1):
                gap = cum[:, h : h + 1] - cum_t[h : h + 1, :]
                lag = jnp.exp(jnp.where(causal, gap, -1e30))
                both.append(
                    jnp.dot(
                        (aff * lag).astype(bf16), xs16[:, at_pair], preferred_element_type=f32
                    )
                )
            y_ref[at, at_pair] = yy[:, at_pair] + jnp.where(near, both[0], both[1])
        fresh = lax.dot_general(
            bb,
            (xs * widen(jnp.exp(last - cum))).astype(bf16),
            (((0,), (0,)), ((), ())),
            preferred_element_type=f32,
        )
        state_ref[...] = state_ref[...] * widen(jnp.exp(last)) + fresh
        base = base_ref[0:1, :]
        efs_ref[at, :] = jnp.exp(base + cum)
        base_ref[0:1, :] = base + last
        return carry

    lax.fori_loop(0, blocks, scan_block, 0)
    st_send[...] = state_ref[...].astype(bf16)
    dec_send[...] = jnp.broadcast_to(base_ref[0:1, :], dec_send.shape)
    odd = me % 2
    partner = me + 1 - 2 * odd

    pairs = planes // 2
    own_pair = z // 2

    def state_copy(src, src_dec, at, sent, device):
        return [
            remote(a, o.at[at], st_ssem.at[sent, i], st_rsem.at[at, i], device)
            for i, (a, o) in enumerate(((src, st_recv), (src_dec, dec_recv)))
        ]

    beside_copies = state_copy(st_send, dec_send, 0, 0, (partner, mt))
    mate_copies = state_copy(pair_send, pair_dec, 1, 1, dev(mate, x, y, c))

    def quad_copies(j, side):
        to = jnp.minimum(2 * j + side, planes - 1)
        return state_copy(pair_send, pair_dec, 2 + own_pair, 2 + 2 * j + side, dev(to, x, y, c))

    for copy in beside_copies:
        copy.start()
    for copy in beside_copies:
        copy.wait_recv()
    own_dec = widen(jnp.exp(dec_send[0:1, :]))
    beside_dec = widen(jnp.exp(dec_recv[0, 0:1, :]))
    beside = st_recv[0].astype(f32)
    later = odd == 1
    plane_state = jnp.where(
        later, state_ref[...] + beside * own_dec, state_ref[...] * beside_dec + beside
    )

    @pl.when(b == 0)
    def _():
        pair_send[...] = plane_state.astype(bf16)
        pair_dec[...] = dec_send[...] + dec_recv[0]
        for copy in mate_copies:
            copy.start()

    @pl.when(b == 1)
    def _():
        for copy in mate_copies:
            copy.wait_recv()
        plane_dec = dec_send[...] + dec_recv[0]
        pair_send[...] = (
            st_recv[1].astype(f32) * widen(jnp.exp(plane_dec[0:1, :])) + plane_state
        ).astype(bf16)
        pair_dec[...] = plane_dec + dec_recv[1]
        for j in range(1, pairs):
            for side in (1, 0):

                @pl.when(own_pair < j)
                def _(j=j, side=side):
                    for copy in quad_copies(j, side):
                        copy.start()

    state_ref[...] = jnp.zeros_like(state_ref)
    send_z(both([1, 2]), free)
    send_xo(range(2, len(units)))

    def join(at):
        state_ref[...] = state_ref[...] * widen(jnp.exp(dec_recv[at, 0:1, :])) + st_recv[at].astype(f32)

    for j in range(pairs - 1):

        @pl.when(own_pair > j)
        def _(j=j):
            for copy in state_copy(pair_send, pair_dec, 2 + j, 0, dev(mate, x, y, c)):
                copy.wait_recv()
            join(2 + j)

    @pl.when(b == 1)
    def _():
        join(1)

    @pl.when(odd == 1)
    def _():
        join(0)

    for copy in late:
        copy.wait()

    def project_block(i, carry):
        at = pl.ds(pl.multiple_of(i * BLOCK, BLOCK), BLOCK)
        yy = y_ref[at, :] + jnp.dot(
            c_act[at, :], state_ref[...].astype(bf16), preferred_element_type=f32
        ) * widen(efs_ref[at, :])
        gated = yy * silu(rv_ref[at, :].astype(f32))
        gated = gated * lax.rsqrt(jnp.mean(gated * gated, axis=-1, keepdims=True) + EPSILON)
        y_norm = (gated * csv_ref[...]).astype(bf16)
        part[at, :] = jnp.dot(y_norm, mm_ref[...], preferred_element_type=f32).astype(bf16)
        return carry

    def rows_of(t):
        return pl.ds(pl.multiple_of(t * own_rows, own_rows), own_rows)

    def near_copy(py):
        return remote(
            part.at[rows_of(py * 2 + 1 - c)],
            near_recv.at[py],
            a_send.at[py],
            a_recv.at[py],
            dev(z, x, y, 1 - c),
        )

    halfway = blocks // 2
    lax.fori_loop((1 - y) * halfway, (2 - y) * halfway, project_block, 0)
    near_copy(1 - y).start()
    lax.fori_loop(y * halfway, (y + 1) * halfway, project_block, 0)
    near_copy(y).start()

    strips = 2
    strip = own_rows // strips

    def side_copy(k):
        at = pl.ds(k * strip, strip)
        return remote(
            side_send.at[at], side_recv.at[at], b_send.at[k], b_recv.at[k], dev(z, x, 1 - y, c)
        )

    near_copy(1 - y).wait_recv()
    for k in range(strips):
        away = pl.ds(pl.multiple_of(((1 - y) * 2 + c) * own_rows + k * strip, strip), strip)
        side_send[k * strip : (k + 1) * strip, :] = (
            part[away, :].astype(f32) + near_recv[1 - y, k * strip : (k + 1) * strip, :].astype(f32)
        ).astype(bf16)
        side_copy(k).start()
    near_copy(y).wait_recv()
    relay_col(0)

    def ag_copies(k):
        lo = pl.ds(k * strip, strip)
        to = normed.at[pl.ds(pl.multiple_of(RIM + mt * own_rows + k * strip, RIM), strip)]
        return [
            remote(own_norm.at[lo], to, ag_send.at[i, k], ag_recv.at[mt, k], device)
            for i, device in enumerate((dev(mate, x, y, b), dev(z, x, 1 - y, b), dev(z, x, y, b)))
        ]

    for k in range(strips):
        side_copy(k).wait_recv()
        lo = slice(k * strip, (k + 1) * strip)
        mine = pl.ds(pl.multiple_of(mt * own_rows + k * strip, strip), strip)
        mixer = (
            part[mine, :].astype(f32)
            + near_recv[y, lo, :].astype(f32)
            + side_recv[lo, :].astype(f32)
        )
        own_norm[lo, :] = layer_norm(
            ALPHA * res_ref[lo, :].astype(f32) + mixer, g1_ref[...]
        ).astype(bf16)
        copies = ag_copies(k)
        copies[0].start()
        copies[1].start()

        @pl.when(c != b)
        def _(copies=copies):
            copies[2].start()

        @pl.when(c == b)
        def _(k=k, lo=lo):
            normed[pl.ds(pl.multiple_of(RIM + mt * own_rows + k * strip, RIM), strip), :] = own_norm[
                lo, :
            ]

    nxt = me + 1
    nz, nx = nxt // FAN, nxt % FAN
    tail = jnp.logical_and(mt == n_tp - 1, nxt < n_sp)
    halo_copies = [
        remote(
            own_norm.at[pl.ds(own_rows - RIM, RIM)],
            normed.at[pl.ds(0, RIM)],
            halo_send.at[i],
            halo_recv,
            dev(jnp.minimum(nz, planes - 1) // 2 * 2 + i // 2, nx, i % 2, nz % 2),
        )
        for i in range(4)
    ]

    @pl.when(tail)
    def _():
        for copy in halo_copies:
            copy.start()

    send_z(both([1, 2]), held)
    send_z(both([3]))
    outer = jnp.logical_or(z == 0, z == planes - 1)
    def far_outer(to):
        return jnp.logical_and(outer, jnp.abs(to - z) > 1)

    send_z(both(shrink), lambda to: jnp.logical_not(far_outer(to)))

    def gathered(t, k):
        here = normed.at[pl.ds(pl.multiple_of(RIM + t * own_rows + k * strip, RIM), strip)]
        return remote(here, here, ag_send.at[0, 0], ag_recv.at[t, k], dev(z, x, y, 1 - c))

    def passed_on(pc, k):
        here = normed.at[pl.ds(pl.multiple_of(RIM + (y * 2 + pc) * own_rows + k * strip, RIM), strip)]
        return remote(here, here, agr_send.at[pc, k], ag_recv.at[y * 2 + pc, k], dev(z, x, 1 - y, c))

    seg = (pair0 + c) * FAN + x

    relay_col(1)

    @pl.when(c != b)
    def _():
        for k in range(strips):
            for pc in range(2):
                gathered(y * 2 + pc, k).wait_recv()
                passed_on(pc, k).start()

    relay_col(2)
    relay_col(3)
    @pl.when(seg == 0)
    def _():
        normed[0:RIM, :] = jnp.zeros((RIM, width), bf16)

    @pl.when(seg > 0)
    def _():
        halo_copies[0].wait_recv()

    for k in range(strips):

        @pl.when(c == b)
        def _(k=k):
            gathered(y * 2 + 1 - c, k).wait_recv()

        for pc in range(2):
            gathered((1 - y) * 2 + pc, k).wait_recv()

    for u in range(3):
        relay_x(u)

    @pl.when(c == b)
    def _():
        for copy in own_copies:
            copy.wait()

    for copy in tap_copies:
        copy.wait()
    same = c == b

    def conv_cols(at, weights, taps, others):
        proj = jnp.dot(normed[...], weights[:, at], preferred_element_type=f32)
        proj = proj.astype(bf16).astype(f32)
        tap = jnp.where(same, taps[:, at].astype(f32), others[:, at].astype(f32))
        total = jnp.zeros((rows, proj.shape[1]), f32)
        for k in range(FCONV):
            start = RIM - (FCONV - 1) + k
            total = total + tap[k : k + 1] * proj[start : start + rows, :]
        return total

    def gate_cols(at):
        gate_act[:, at] = silu(conv_cols(at, v_all, vk_ref, vk_other))

    def up_cols(at):
        hidden[:, at] = (gate_act[:, at] * conv_cols(at, w_all, wk_ref, wk_other)).astype(bf16)

    chunk = 256
    full = ff // chunk

    def run_cols(fn, lo, hi):
        def one(i, carry):
            fn(pl.ds(pl.multiple_of(i * chunk, chunk), chunk))
            return carry

        lax.fori_loop(lo, hi, one, 0)

    def rest_cols(fn):
        if ff % chunk:
            fn(pl.ds(full * chunk, ff % chunk))

    complete(0)
    run_cols(gate_cols, 0, full)
    rest_cols(gate_cols)
    send_z(both(shrink), lambda to: jnp.logical_and(far_outer(to), to < z))
    relay_x(3)
    complete(1)

    def relay_s(i):
        for u in shrink:
            relay_col(u, [i])

    relay_s(1)
    run_cols(up_cols, 0, full // 2)
    relay_s(2)
    run_cols(up_cols, full // 2, full - 1)
    send_z(both(shrink), lambda to: jnp.logical_and(far_outer(to), to > z))
    run_cols(up_cols, full - 1, full)
    rest_cols(up_cols)

    def down(who):
        at = pl.ds(pl.multiple_of(who * cols, cols), cols)
        part[:, at] = jnp.dot(
            hidden[...], s_all[who], preferred_element_type=f32
        ).astype(bf16)

    def at_of(who):
        return pl.ds(pl.multiple_of(who * cols, cols), cols)

    def side_half(py):
        return pl.ds(pl.multiple_of(py * 2 * own_rows, own_rows), 2 * own_rows)

    def home_copies(who):
        at = at_of(who)
        return [
            remote(
                part.at[rows_of(py * 2 + pc), at],
                recv2.at[y, :, at],
                t3_send,
                t3_recv.at[y],
                dev(z, x, py, pc),
            )
            for py, pc in ((1 - y, 0), (1 - y, 1), (y, 1 - c))
        ]

    def cross_copy(who):
        at = at_of(who)
        return remote(
            part.at[side_half(1 - y), at], pre_recv.at[:, at], p_send, p_recv.at[who], dev(z, x, 1 - y, c)
        )

    def away_copies(who):
        at = at_of(who)
        return [
            remote(
                part.at[rows_of(y * 2 + pc), at],
                recv2.at[2, :, at],
                t3_send,
                t3_recv.at[2],
                dev(mate, x, y, pc),
            )
            for pc in range(2)
        ]

    done = []
    lag = 2

    def finish(who):
        at = at_of(who)

        @pl.when(c != b)
        def _():
            cross_copy(who).wait_recv()
            here = side_half(y)
            part[here, at] = (part[here, at].astype(f32) + pre_recv[:, at].astype(f32)).astype(bf16)
            for copy in away_copies(who):
                copy.start()

    def down_step(who):
        down(who)
        at = at_of(who)

        @pl.when(c != b)
        def _():
            cross_copy(who).start()

        @pl.when(c == b)
        def _():
            for copy in home_copies(who):
                copy.start()
            recv2[y, :, at] = part[rows_of(mt), at]

        done.append(who)
        if len(done) > lag:
            finish(done[-1 - lag])

    near_copy(0).wait_send()
    near_copy(1).wait_send()

    @pl.when(c != b)
    def _():
        arrived(ds_recv.at[me], depth)

    down_step(me)

    def x_step(i):
        who = plane_at(i) * FAN + 1 - x
        relay_xs(i)
        arrived(ds_recv.at[who], depth // 2)
        down_step(who)

    def col_step(i):
        who = plane_at(i) * FAN + x
        arrived(ds_recv.at[who], depth // 2)
        down_step(who)

    x_step(0)
    col_step(1)
    last = planes - 1
    relay_col(4, [last])
    relay_col(5, [last])
    x_step(1)
    relay_col(6, [last])
    for i in range(2, last):
        col_step(i)
        if i == 2:
            relay_col(7, [last])
        x_step(i)
    col_step(last)
    x_step(last)
    for who in done[-lag:]:
        finish(who)

    for t in range(3):

        @pl.when(jnp.logical_or(c != b, y != t))
        def _(t=t):
            remote(recv2.at[t], recv2.at[t], t3_send, t3_recv.at[t], dev(z, x, y, 1 - c)).wait_recv()

    channel = recv2[0].astype(f32)
    for t in range(1, 3):
        channel = channel + recv2[t].astype(f32)
    out_ref[...] = layer_norm(
        ALPHA * own_norm[...].astype(f32) + channel, g2_ref[...]
    ).astype(bf16)

    def part_left(sem, count):
        here = part.at[pl.ds(0, count)]
        remote(here, here, sem, t3_recv.at[0], dev(z, x, y, 1 - c)).wait_send()

    @pl.when(c == b)
    def _():
        part_left(t3_send, 3 * own_rows)
        left(xo_send, 3 * depth)
        left(do_send, 3 * depth)

    @pl.when(c != b)
    def _():
        part_left(t3_send, 2 * own_rows)
        part_left(p_send, 2 * own_rows)

    half_blocks = 3 * depth // 2
    left(xr_send, (planes - 1) * half_blocks)
    left(dr_send.at[0], (planes - 1) * half_blocks)
    left(dr_send.at[1], planes * half_blocks)
    for j in range(dests):

        @pl.when(2 * j + c != z)
        def _(j=j):
            left(z_send.at[j], 3 * depth)

    for copy in rim_copies:
        copy.wait_send()
    for k in range(strips):
        side_copy(k).wait_send()
        copies = ag_copies(k)
        copies[0].wait_send()
        copies[1].wait_send()

        @pl.when(c != b)
        def _(k=k, copies=copies):
            copies[2].wait_send()
            for pc in range(2):
                passed_on(pc, k).wait_send()

    @pl.when(tail)
    def _():
        for copy in halo_copies:
            copy.wait_send()

    for copy in beside_copies:
        copy.wait_send()

    @pl.when(b == 0)
    def _():
        for copy in mate_copies:
            copy.wait_send()

    for j in range(1, pairs):
        for side in range(2):

            @pl.when(jnp.logical_and(b == 1, own_pair < j))
            def _(j=j, side=side):
                for copy in quad_copies(j, side):
                    copy.wait_send()


def fused_shards(n_sp, n_tp, *args):
    (
        res, rv, xf, bf, cf, dt, doff, fade, elf, byp, xk, bk, ck, csv, mm, g1, v, w, s, vk, wk, g2
    ) = args
    f32, bf16 = jnp.float32, jnp.bfloat16
    rows, inner = xf.shape
    heads = dt.shape[1]
    width = mm.shape[1]
    ff = v.shape[1]
    own_rows = rows // n_tp
    row = lambda a: a.reshape(1, -1)
    half = n_sp // 2
    planes = n_sp // FAN
    units = sum(CUTS)
    vmem = pl.BlockSpec(memory_space=pltpu.VMEM)
    hbm = pl.BlockSpec(memory_space=pl.ANY)
    dma = pltpu.SemaphoreType.DMA
    return pl.pallas_call(
        functools.partial(layer_kernel, n_sp, n_tp),
        out_shape=jax.ShapeDtypeStruct(res.shape, bf16),
        in_specs=[hbm] * 2 + [vmem] * 12 + [hbm, vmem] + [hbm] * 3 + [vmem] * 3,
        out_specs=vmem,
        scratch_shapes=[
            pltpu.VMEM((n_sp * v.shape[0], ff), bf16),
            pltpu.VMEM((n_sp * v.shape[0], ff), bf16),
            pltpu.VMEM((n_sp,) + s.shape, bf16),
            pltpu.VMEM((RIM, inner), bf16),
            pltpu.VMEM((RIM, STATE), bf16),
            pltpu.VMEM((RIM, STATE), bf16),
            pltpu.VMEM(vk.shape, bf16),
            pltpu.VMEM(wk.shape, bf16),
            pltpu.VMEM((rows + RIM, 128), f32),
            pltpu.VMEM((rows, inner), bf16),
            pltpu.VMEM((rows, STATE), bf16),
            pltpu.VMEM((rows, STATE), bf16),
            pltpu.VMEM((heads, rows), f32),
            pltpu.VMEM((heads, rows), f32),
            pltpu.VMEM((rows, inner), f32),
            pltpu.VMEM((rows, heads), f32),
            pltpu.VMEM((8, heads), f32),
            pltpu.VMEM((STATE, inner), f32),
            pltpu.VMEM((STATE, inner), bf16),
            pltpu.VMEM((8, heads), f32),
            pltpu.VMEM((STATE, inner), bf16),
            pltpu.VMEM((8, heads), f32),
            pltpu.VMEM((half, STATE, inner), bf16),
            pltpu.VMEM((half, 8, heads), f32),
            pltpu.VMEM((rows, width), bf16),
            pltpu.VMEM((2, own_rows, width), bf16),
            pltpu.VMEM((own_rows, width), bf16),
            pltpu.VMEM((own_rows, width), bf16),
            pltpu.VMEM((own_rows, width), bf16),
            pltpu.VMEM((3, own_rows, width), bf16),
            pltpu.VMEM((2 * own_rows, width), bf16),
            pltpu.VMEM((rows + RIM, width), bf16),
            pltpu.VMEM((rows, ff), f32),
            pltpu.VMEM((rows, ff), bf16),
            pltpu.VMEM(res.shape, bf16),
            pltpu.VMEM(rv.shape, bf16),
            pltpu.VMEM(mm.shape, bf16),
            dma((3,)),
            dma((3,)),
            dma((units, planes)),
            dma((CUTS[0] + CUTS[1],)),
            dma((planes,)),
            dma((2,)),
            dma((n_sp,)),
            dma((planes // 2,)),
            dma,
            dma,
            dma,
            dma((2,)),
            dma((3,)),
            dma((3,)),
            dma((2,)),
            dma((2,)),
            dma((2 + planes, 2)),
            dma((half, 2)),
            dma((2,)),
            dma((2,)),
            dma((2,)),
            dma((2,)),
            dma((3, 2)),
            dma((n_tp, 2)),
            dma((2, 2)),
            dma((4,)),
            dma,
            dma,
            dma((3,)),
            dma,
            dma((n_sp,)),
        ],
        compiler_params=pltpu.CompilerParams(
            collective_id=0, has_side_effects=True, vmem_limit_bytes=60 * 1024 * 1024
        ),
    )(
        res, rv, xf, bf, cf, dt.T, row(doff), row(fade), elf.T, row(byp), xk, bk, ck, row(csv), mm,
        row(g1), v, w, s, vk, wk, row(g2),
    )


def shards_for(n_sp, n_tp):
    def shards(*args):
        rows = args[2].shape[0]
        fits = (
            args[3].shape[1] == STATE
            and args[18].shape[1] % 128 == 0
            and args[16].shape[0] % 64 == 0
            and args[16].shape[1] % 128 == 0
            and n_sp % (2 * FAN) == 0
            and n_sp > 2 * FAN
            and n_tp == 4
            and args[18].shape[0] % 128 == 0
            and args[18].shape[::-1] == args[16].shape
            and rows % (BLOCK * n_tp) == 0
        )
        if fits:
            return fused_shards(n_sp, n_tp, *args)
        return plain_shards(*args)

    return shards


def solution(mesh):
    in_specs = (
        P(("sp", "tp"), None),
        P("sp", "tp"),
        P("sp", "tp"),
        P("sp", "tp"),
        P("sp", "tp"),
        P("sp", "tp"),
        P("tp"),
        P("tp"),
        P("sp", "tp"),
        P("tp"),
        P(None, "tp"),
        P(None, "tp"),
        P(None, "tp"),
        P("tp"),
        P("tp", None),
        P(),
        P("sp", "tp"),
        P("sp", "tp"),
        P("tp", "sp"),
        P(None, "tp"),
        P(None, "tp"),
        P(),
    )
    out_specs = P(("sp", "tp"), None)
    shards = shards_for(mesh.shape["sp"], mesh.shape["tp"])
    return jax.shard_map(shards, mesh=mesh, in_specs=in_specs, out_specs=out_specs, check_vma=False)
```
